256 devices in a mesh: sp: 64 (over z, y, core), tp: 4 (over x).
Axes of the slice: x: 4, y: 4, z: 8, core: 2. Of those that a mesh axis runs over, the one named last changes fastest.
Arguments:
- queries: bfloat16 [12288, 2048], P('sp', 'tp'), may hold values from -100 to 100
- keys: bfloat16 [12288, 512], P('sp'), may hold values from -8 to 8
- values: bfloat16 [12288, 512], P('sp'), may hold values from -6 to 6
- diff_scale: float32 [8], P('tp'), may hold values from 0.3 to 0.8
- head_gain: float32 [256], replicated, may hold values from 0.1 to 1.9
- w_out: bfloat16 [2048, 2048], P('tp'), may hold values from -0.125 to 0.125
- residual: bfloat16 [12288, 2048], P(('sp', 'tp')), may hold values from -6 to 6
- norm_gain: float32 [2048], replicated, may hold values from 0.1 to 1.9
- route_ids: int32 [12288, 2], P(('sp', 'tp')), may hold values from 0 to 63, all different within a row; in each aligned block of 48 rows (0 to 47, 48 to 95, ...) at most 2 rows name the same one
- route_weights: float32 [12288, 2], P(('sp', 'tp')), may hold values from 0.2 to 1
- w_gate: bfloat16 [64, 2048, 3072], P('sp', None, 'tp'), may hold values from -0.125 to 0.125
- w_up: bfloat16 [64, 2048, 3072], P('sp', None, 'tp'), may hold values from -0.125 to 0.125
- w_down: bfloat16 [64, 3072, 2048], P('sp', 'tp'), may hold values from -0.109375 to 0.109375
Outputs:
- layer_out: bfloat16 [12288, 2048], P(('sp', 'tp'))
The draws below stay inside these ranges and needn't reach their ends.
Inputs may be any that keep to these rules, and one draw needn't show every extreme that they name: `route_ids`: in each aligned block of 48 rows (the rows of one device), no expert is named more than 2 times, a bound that some block reaches; a row names 2 different experts.
All inputs are finite; a program needn't handle non-finite values.
Results may differ from the reference program's by a relative error of at most 0.014.
Values may be sent and summed in bfloat16 or wider, within the bound.
No kernel may reach another device: no remote copies, remote signals or barrier semaphores. Data moves between devices by JAX's collectives and lax.ppermute only.
A program may use at most 128 MiB of HBM per device.

```python
import math
import jax
import jax.numpy as jnp
import numpy as np
from jax import lax

HEAD_DIM = 128
V_DIM = 256
HEADS = 8
KV_HEADS = 2
D = 2048
FF = 3072
TOP = 2
TOKENS = 12288
ROWS = 48
FF_DEV = 768
EXPERTS = 64
CAP = 2
N_TP = 4


def paired(key):
    base = jax.random.fold_in(key, 11)
    key_q, key_k = jax.random.split(base, 2)
    queries = jnp.clip(jax.random.normal(key_q, (TOKENS, HEADS * 2 * HEAD_DIM), jnp.float32) * 1.3, -8.0, 8.0)
    keys = jnp.clip(jax.random.normal(key_k, (TOKENS, KV_HEADS * 2 * HEAD_DIM), jnp.float32) * 1.3, -8.0, 8.0)
    return (queries, keys)


def draw_queries(key, part):
    return paired(key)[0].astype(jnp.bfloat16)


def draw_keys(key, part):
    return paired(key)[1].astype(jnp.bfloat16)


def block_levels(key, shape, shards, low, largest):
    factor_of, own = 1.0, jax.random.fold_in(key, 6)
    for dim, blocks in shards:
        steps = jnp.exp(jax.random.uniform(jax.random.fold_in(own, dim), (blocks,), jnp.float32, low / len(shards), largest / len(shards)))
        factor_of = factor_of * jnp.repeat(steps, shape[dim] // blocks).reshape([-1 if axis == dim else 1 for axis in range(len(shape))])
    return factor_of


def assign_block(own_key, own, number, rows, amount, top, bound, slope):
    sequence = jax.random.permutation(own_key, amount)
    packed, ordinary = shares(amount, rows * top, bound, slope, True), shares(amount, rows * top, bound, slope, False)
    places = jnp.arange(amount)

    def named(tallies, turn):
        used = int((tallies > 0).sum())
        fixed = max(1, used // 4)
        passed = fixed + (places - fixed + turn * (used - fixed)) % max(1, amount - fixed)
        return jnp.zeros((amount,), jnp.int32).at[sequence[jnp.where(places < fixed, places, passed)]].set(jnp.asarray(tallies, jnp.int32))

    tallies = jnp.where(number % 4 == 0, named(packed, number // 4), named(ordinary, number - number // 4 - 1))
    mixed = jax.random.permutation(jax.random.fold_in(own, 3), amount)
    donor, taker = mixed[0:amount // 2 * 2:2], mixed[1:amount // 2 * 2:2]
    slack = jnp.minimum(tallies[donor] - 1, bound - tallies[taker]) // 2
    slack = jnp.where((donor == sequence[0]) | (taker == sequence[0]) | (tallies[taker] == 0), 0, jnp.maximum(slack, 0))
    passed = jax.random.randint(jax.random.fold_in(own, 4), (amount // 2,), 0, 1 << 20) % (slack + 1)
    tallies = tallies.at[donor].add(-passed).at[taker].add(passed)
    labels = jnp.searchsorted(jnp.cumsum(tallies), jnp.arange(rows * top), side="right").astype(jnp.int32)
    table = labels.reshape(top, rows).T
    table = table[jax.random.permutation(jax.random.fold_in(own, 1), rows)]
    turn = jax.random.randint(jax.random.fold_in(own, 2), (rows, 1), 0, top)
    return jnp.take_along_axis(table, (jnp.arange(top)[None, :] + turn) % top, axis=1)


def shares(amount, total, limit, skew, full):
    portions = [(1 << 20) // math.isqrt(rank ** skew) + 1 for rank in range(1, amount + 1)]
    largest = limit if full else min(limit, max(-(-total // amount), total * portions[0] // sum(portions)))
    least = 1 if total - largest >= amount - 1 else 0
    counts, rest = [largest] + [least] * (amount - 1), total - largest - least * (amount - 1)
    while rest > 0:
        movable = [i for i in range(1, amount) if counts[i] < largest] or [i for i in range(1, amount) if counts[i] < limit]
        pool, left = sum([portions[i] for i in movable]), rest
        for i in movable:
            addition = min(limit - counts[i], max(1, left * portions[i] // pool), rest)
            counts[i] = counts[i] + addition
            rest = rest - addition
    return np.array(counts)


def centred(own_key, shape, width, bound, pieces=(), held_as=jnp.bfloat16):
    drawn = jax.random.normal(own_key, shape, jnp.float32) * width
    if len(pieces) > 0:
        drawn = block_levels(own_key, shape, pieces, -0.22, 0.18) * drawn
    return jnp.clip(drawn, min=-bound, max=bound).astype(held_as)


def setup_inputs(seed: int = 0) -> dict:
    key_of = jax.random.split(jax.random.key(seed), 14)
    queries = draw_queries(jax.random.fold_in(key_of[13], 71), 0)
    keys = draw_keys(jax.random.fold_in(key_of[13], 71), 0)
    values = centred(key_of[2], (TOKENS, KV_HEADS * V_DIM), 1.0, 6.0, ((0, 64),))
    diff_scale = jnp.clip(0.3 + 0.5 * jax.random.uniform(key_of[3], (HEADS,), jnp.float32) ** block_levels(key_of[3], (HEADS,), ((0, 4),), -0.2, 0.2), 0.3, 0.8)
    head_gain = jnp.clip(1.0 + 0.18 * jax.random.normal(key_of[4], (V_DIM,), jnp.float32), 0.1, 1.9)
    w_out = centred(key_of[5], (HEADS * V_DIM, D), (HEADS * V_DIM) ** -0.5, 0.125, ((0, 4),))
    residual = centred(key_of[6], (TOKENS, D), 1.0, 6.0, ((0, 256),))
    norm_gain = jnp.clip(1.0 + 0.18 * jax.random.normal(key_of[7], (D,), jnp.float32), 0.1, 1.9)
    route_ids_keys = jax.random.split(jax.random.fold_in(key_of[8], 1), TOKENS // ROWS)
    route_ids_turns = jax.random.permutation(jax.random.fold_in(key_of[8], 3), TOKENS // ROWS)
    route_ids = jax.vmap(lambda own, number: assign_block(jax.random.fold_in(key_of[8], 2), own, number, ROWS, EXPERTS, TOP, CAP, 1))(route_ids_keys, route_ids_turns).reshape((TOKENS, TOP))
    route_weights = jnp.clip(0.2 + 0.8 * jax.random.uniform(key_of[9], (TOKENS, TOP), jnp.float32) ** block_levels(key_of[9], (TOKENS, TOP), ((0, 256),), -0.2, 0.2), 0.2, 1.0)
    w_gate = centred(key_of[10], (EXPERTS, D, FF), D ** -0.5, 0.125, ((0, 64), (2, 4)))
    w_up = centred(key_of[11], (EXPERTS, D, FF), D ** -0.5, 0.125, ((0, 64), (2, 4)))
    w_down = centred(key_of[12], (EXPERTS, FF, D), FF ** -0.5, 0.109375, ((0, 64), (1, 4)))
    return {"queries": queries, "keys": keys, "values": values, "diff_scale": diff_scale, "head_gain": head_gain, "w_out": w_out, "residual": residual, "norm_gain": norm_gain, "route_ids": route_ids, "route_weights": route_weights, "w_gate": w_gate, "w_up": w_up, "w_down": w_down}


EPS = 1e-06

def rounded(value):
    return lax.optimization_barrier(value.astype(jnp.bfloat16)).astype(jnp.float32)

def reference(queries, keys, values, diff_scale, head_gain, w_out, residual, norm_gain, route_ids, route_weights, w_gate, w_up, w_down):
    q_heads = queries.reshape(TOKENS, HEADS, 2, HEAD_DIM)
    k_groups = keys.reshape(TOKENS, KV_HEADS, 2, HEAD_DIM).astype(jnp.float32)
    v_groups = values.reshape(TOKENS, KV_HEADS, V_DIM).astype(jnp.float32)
    block = math.gcd(TOKENS, 512)
    per_group = HEADS // KV_HEADS

    def attend_block(q_block):
        outs = []
        for head in range(HEADS):
            grp = head // per_group
            scores = jnp.einsum('qmd,kmd->mqk', q_block[:, head].astype(jnp.float32), k_groups[:, grp]) / math.sqrt(HEAD_DIM)
            peak = lax.optimization_barrier(jnp.max(scores, axis=-1, keepdims=True))
            weights = rounded(jnp.exp(scores - peak))
            totals = lax.optimization_barrier(jnp.sum(weights, axis=-1))
            numer = jnp.einsum('mqk,kd->mqd', weights, v_groups[:, grp])
            outs.append(numer[0] / totals[0][:, None] - diff_scale[head] * numer[1] / totals[1][:, None])
        mixed = jnp.stack(outs, axis=1)
        normal_part = mixed * lax.rsqrt(lax.optimization_barrier(jnp.mean(mixed * mixed, axis=-1, keepdims=True)) + EPS) * head_gain
        return normal_part.astype(jnp.bfloat16).reshape(block, HEADS * V_DIM)
    head_out = lax.map(attend_block, q_heads.reshape(TOKENS // block, block, HEADS, 2, HEAD_DIM)).reshape(TOKENS, HEADS * V_DIM)
    width_dev = HEADS * V_DIM // N_TP
    attended = jnp.zeros((TOKENS, D), jnp.float32)
    for part in range(N_TP):
        attended = attended + rounded(jnp.dot(head_out[:, part * width_dev:(part + 1) * width_dev], w_out[part * width_dev:(part + 1) * width_dev], preferred_element_type=jnp.float32))
    state = residual.astype(jnp.float32) + attended
    normed = (state * lax.rsqrt(lax.optimization_barrier(jnp.mean(state * state, axis=-1, keepdims=True)) + EPS) * norm_gain).astype(jnp.bfloat16)
    blocks = TOKENS // ROWS
    ids = route_ids.reshape(blocks, ROWS * TOP)
    onehot = (ids[:, :, None] == jnp.arange(EXPERTS, dtype=jnp.int32)[None, None, :]).astype(jnp.int32)
    slot = lax.optimization_barrier(jnp.sum((jnp.cumsum(onehot, axis=1) - onehot) * onehot, axis=-1))
    dest = (ids * (blocks * CAP) + jnp.arange(blocks, dtype=jnp.int32)[:, None] * CAP + slot).reshape(-1).astype(jnp.int32)
    copies = jnp.repeat(normed, TOP, axis=0)
    buffer = jnp.zeros((EXPERTS * blocks * CAP, D), jnp.bfloat16).at[dest].set(copies).reshape(EXPERTS, blocks * CAP, D)

    def serve(inputs):
        rows_in, gate_w, up_w, down_w = inputs
        gate = jnp.dot(rows_in, gate_w, preferred_element_type=jnp.float32)
        up = jnp.dot(rows_in, up_w, preferred_element_type=jnp.float32)
        hidden = (jax.nn.silu(gate) * up).astype(jnp.bfloat16)
        summed = jnp.zeros((rows_in.shape[0], D), jnp.float32)
        for part in range(N_TP):
            summed = summed + rounded(jnp.dot(hidden[:, part * FF_DEV:(part + 1) * FF_DEV], down_w[part * FF_DEV:(part + 1) * FF_DEV], preferred_element_type=jnp.float32))
        return summed.astype(jnp.bfloat16)
    served = lax.map(serve, (buffer, w_gate, w_up, w_down)).reshape(-1, D)
    picked = served[dest].reshape(TOKENS, TOP, D)
    expert_sum = jnp.einsum('rt,rtd->rd', route_weights.astype(jnp.float32), picked.astype(jnp.float32))
    return (state + expert_sum).astype(jnp.bfloat16)
```

```python
import functools
import math

import jax
import jax.numpy as jnp
from jax import lax
from jax.experimental import pallas as pl
from jax.experimental.pallas import tpu as pltpu
from jax.sharding import Mesh
from jax.sharding import PartitionSpec as P

KV_HEADS = 2
SP = ("z", "y", "core")
TP = ("xh", "xl")


EPS = 1e-06
LOG2E = math.log2(math.e)


def cut_along(shard, dim, peers):
    before, after = (shard.shape[:dim], shard.shape[dim + 1 :])
    return jnp.moveaxis(shard.reshape(*before, peers, -1, *after), dim, 0)


def sent_and_summed(shard, axis, dim):
    pieces = cut_along(shard, dim, lax.axis_size(axis))
    arrived = lax.all_to_all(pieces, axis, split_axis=0, concat_axis=0, tiled=True)
    return arrived.astype(jnp.float32).sum(axis=0)


def copy_for_each(shard, axis):
    copies = jnp.broadcast_to(shard, (lax.axis_size(axis), *shard.shape))
    return lax.all_to_all(copies, axis, split_axis=0, concat_axis=0, tiled=True)


def joined_along(pieces, dim):
    pieces = jnp.moveaxis(pieces, 0, dim)
    dims = pieces.shape
    return pieces.reshape(*dims[:dim], dims[dim] * dims[dim + 1], *dims[dim + 2 :])


def gathered_copies(shard, axis, dim):
    pieces = copy_for_each(shard, axis)
    return joined_along(pieces, dim)


def shifted(x, axis, by):
    n = lax.axis_size(axis)
    return lax.ppermute(x, axis, [(i, (i + by) % n) for i in range(n)])


def ring_pieces(block, axis):
    n = lax.axis_size(axis)
    pieces, right, left = [block], block, block
    for _ in range((n - 1) // 2):
        right, left = shifted(right, axis, 1), shifted(left, axis, -1)
        pieces += [right, left]
    half = block.shape[0] // 2
    pieces.append(shifted(right[:half], axis, 1))
    pieces.append(shifted(left[half:], axis, -1))
    return pieces


def direct_pieces(block, axis):
    n = lax.axis_size(axis)
    return [block] + [shifted(block, axis, by) for by in sorted(range(1, n), key=lambda b: -min(b, n - b))]


def attention_kernel(n_kv, scale, q_ref, *refs):
    kv_refs = refs[:n_kv]
    o_ref, stat_ref, k0, k1, v, s_a, s_b, p_a, p_b = refs[n_kv:]
    ks = (k0, k1)
    at = 0
    for ref in kv_refs:
        n = ref.shape[0]
        k0[at : at + n] = ref[:, :128]
        k1[at : at + n] = ref[:, 128:256]
        v[at : at + n] = ref[:, 256:]
        at += n
    pieces, _, rows, _ = q_ref.shape
    sub = 16

    def score(i, m, s):
        s[...] = lax.dot_general(
            q_ref[i, m],
            ks[m][...],
            (((1,), (1,)), ((), ())),
            preferred_element_type=jnp.float32,
        )

    def soft(i, m, s, p):
        lane = lax.broadcasted_iota(jnp.int32, (sub, 128), 1)
        for r in range(0, rows, sub):
            x = s[r : r + sub]
            high = jnp.max(x, axis=1, keepdims=True)
            e = jnp.exp2((x - high) * (scale * LOG2E))
            p[r : r + sub] = e.astype(jnp.bfloat16)
            total = jnp.sum(e, axis=1, keepdims=True)
            stat_ref[i, m, r : r + sub] = jnp.where(lane == 0, high * scale, total)

    def mix(i, m, p):
        o = jnp.dot(p[...], v[...], preferred_element_type=jnp.float32)
        o_ref[i, m] = o.astype(o_ref.dtype)

    score(0, 0, s_a)

    def body(i, _):
        score(i, 1, s_b)

        @pl.when(i > 0)
        def _():
            mix(i - 1, 1, p_b)

        soft(i, 0, s_a, p_a)
        score(jnp.minimum(i + 1, pieces - 1), 0, s_a)
        mix(i, 0, p_a)
        soft(i, 1, s_b, p_b)
        return 0

    lax.fori_loop(0, pieces, body, 0)
    mix(pieces - 1, 1, p_b)


def attention(q, kvs, scale):
    pieces, _, rows, half = q.shape
    n_keys = sum(kv.shape[0] for kv in kvs)
    width = kvs[0].shape[1] - 2 * half
    vmem = pl.BlockSpec(memory_space=pltpu.VMEM)
    return pl.pallas_call(
        functools.partial(attention_kernel, len(kvs), scale),
        out_shape=(
            jax.ShapeDtypeStruct((pieces, 2, rows, width), jnp.bfloat16),
            jax.ShapeDtypeStruct((pieces, 2, rows, 128), jnp.float32),
        ),
        in_specs=[vmem] * (1 + len(kvs)),
        out_specs=(vmem, vmem),
        scratch_shapes=[pltpu.VMEM((n_keys, half), jnp.bfloat16)] * 2
        + [pltpu.VMEM((n_keys, width), jnp.bfloat16)]
        + [pltpu.VMEM((rows, n_keys), jnp.float32)] * 2
        + [pltpu.VMEM((rows, n_keys), jnp.bfloat16)] * 2,
        compiler_params=pltpu.CompilerParams(vmem_limit_bytes=48 * 1024 * 1024),
        name="attention",
    )(q, *kvs)


def merged(a, b):
    oa, ha, ta = a
    ob, hb, tb = b
    high = jnp.maximum(ha, hb)
    fa, fb = jnp.exp(ha - high), jnp.exp(hb - high)
    o = oa.astype(jnp.float32) * fa[..., None] + ob.astype(jnp.float32) * fb[..., None]
    return o, high, ta * fa + tb * fb


def swapped(part, axis):
    o, high, total = part
    perm = [(0, 1), (1, 0)]
    stats = lax.ppermute(jnp.stack([high, total]), axis, perm)
    return lax.ppermute(o.astype(jnp.bfloat16), axis, perm), stats[0], stats[1]


def local(
    queries,
    keys,
    values,
    diff_scale,
    head_gain,
    w_out,
    residual,
    norm_gain,
    route_ids,
    route_weights,
    w_gate,
    w_up,
    w_down,
):
    q_rows = queries.shape[0]
    heads_dev = diff_scale.shape[0]
    half_dim = queries.shape[1] // (2 * heads_dev)
    group_cols = keys.shape[1] // KV_HEADS
    value_cols = values.shape[1] // KV_HEADS
    swap = [(0, 1), (1, 0)]

    group, quarter = lax.axis_index("xh"), lax.axis_index("xl")
    part_rows = q_rows // 2
    k_part = lax.dynamic_slice(
        keys, (quarter * part_rows, group * group_cols), (part_rows, group_cols)
    )
    v_part = lax.dynamic_slice(
        values, (quarter * part_rows, group * value_cols), (part_rows, value_cols)
    )
    joined = jnp.concatenate([k_part, v_part], axis=1)
    first, second = joined[: part_rows // 2], joined[part_rows // 2 :]
    q_own = queries.reshape(q_rows, heads_dev, 2, half_dim).transpose(2, 1, 0, 3)
    q_own = q_own.reshape(2, heads_dev * q_rows, half_dim)

    by_z = jnp.concatenate(direct_pieces(first, "y"))
    by_y = jnp.concatenate(direct_pieces(second, "z"))
    pieces = ring_pieces(by_z, "z") + ring_pieces(by_y, "y")
    q_core = lax.ppermute(q_own, "core", swap)
    q_x = lax.ppermute(q_own, "xl", swap)
    q_both = lax.ppermute(q_core, "xl", swap)

    o, stats = attention(
        jnp.stack([q_own, q_core, q_x, q_both]), pieces, 1.0 / math.sqrt(half_dim)
    )
    high, total = stats[..., 0], stats[..., 1]

    def part(i):
        return o[i], high[i], total[i]

    mine = merged(part(0), swapped(part(1), "core"))
    across = merged(part(2), swapped(part(3), "core"))
    acc, high, total = merged(mine, swapped(across, "xl"))

    acc = (acc / total[..., None]).reshape(2, heads_dev, q_rows, value_cols)
    mixed = acc[0] - diff_scale[:, None, None] * acc[1]
    mixed = mixed * lax.rsqrt(jnp.mean(mixed * mixed, axis=-1, keepdims=True) + EPS) * head_gain
    head_out = mixed.astype(jnp.bfloat16).transpose(1, 0, 2)
    head_out = head_out.reshape(q_rows, heads_dev * value_cols)
    rows_out = residual.shape[0]
    attended = sent_and_summed(
        jnp.dot(head_out, w_out, preferred_element_type=jnp.float32).astype(jnp.bfloat16), TP, 0
    )
    state = residual.astype(jnp.float32) + attended
    normed = (
        state * lax.rsqrt(jnp.mean(state * state, axis=-1, keepdims=True) + EPS) * norm_gain
    ).astype(jnp.bfloat16)
    experts = lax.axis_size(SP)
    top = route_ids.shape[1]
    width = normed.shape[1]
    capacity = max(2, 3 * rows_out * top // (2 * experts))
    flat_ids = route_ids.reshape(-1)
    onehot = (flat_ids[:, None] == jnp.arange(experts, dtype=jnp.int32)[None, :]).astype(jnp.int32)
    slot = jnp.sum((jnp.cumsum(onehot, axis=0) - onehot) * onehot, axis=1)
    dest = flat_ids * capacity + slot
    copies = jnp.repeat(normed, top, axis=0)
    outgoing = (
        jnp.zeros((experts * capacity, width), jnp.bfloat16)
        .at[dest]
        .set(copies)
        .reshape(experts, capacity, width)
    )
    gathered = gathered_copies(
        lax.all_to_all(outgoing, SP, split_axis=0, concat_axis=0, tiled=True), TP, 0
    )
    flat = gathered.reshape(-1, width)
    gate = jnp.dot(flat, w_gate[0], preferred_element_type=jnp.float32)
    up = jnp.dot(flat, w_up[0], preferred_element_type=jnp.float32)
    hidden = (jax.nn.silu(gate) * up).astype(jnp.bfloat16)
    partial_value = jnp.dot(hidden, w_down[0], preferred_element_type=jnp.float32).reshape(
        gathered.shape[0], gathered.shape[1], width
    )
    served = sent_and_summed(partial_value.astype(jnp.bfloat16), TP, 0).astype(jnp.bfloat16)
    returned = lax.all_to_all(served, SP, split_axis=0, concat_axis=0, tiled=True).reshape(
        experts * capacity, width
    )
    picked = returned[dest].reshape(rows_out, top, width)
    expert_sum = jnp.einsum("rt,rtd->rd", route_weights, picked.astype(jnp.float32))
    return (state + expert_sum).astype(jnp.bfloat16)


def solution(mesh):
    cells = mesh.devices.reshape(8, 4, 2, 2, 2)
    mesh = Mesh(cells, ("z", "y", "core", "xh", "xl"))
    in_specs = (
        P(SP, TP),
        P(SP, None),
        P(SP, None),
        P(TP),
        P(),
        P(TP, None),
        P(SP + TP, None),
        P(),
        P(SP + TP, None),
        P(SP + TP, None),
        P(SP, None, TP),
        P(SP, None, TP),
        P(SP, TP, None),
    )
    out_specs = P(SP + TP, None)
    return jax.shard_map(local, mesh=mesh, in_specs=in_specs, out_specs=out_specs, check_vma=False)
```

```python
import functools
import math

import jax
import jax.numpy as jnp
from jax import lax
from jax.experimental import pallas as pl
from jax.experimental.pallas import tpu as pltpu
from jax.sharding import Mesh
from jax.sharding import PartitionSpec as P

KV_HEADS = 2
SP = ("z", "y", "core")
TP = ("xh", "xl")


EPS = 1e-06
LOG2E = math.log2(math.e)


def cut_along(shard, dim, peers):
    before, after = (shard.shape[:dim], shard.shape[dim + 1 :])
    return jnp.moveaxis(shard.reshape(*before, peers, -1, *after), dim, 0)


def shifted(x, axis, by):
    n = lax.axis_size(axis)
    return lax.ppermute(x, axis, [(i, (i + by) % n) for i in range(n)])


def ring_pieces(block, axis):
    n = lax.axis_size(axis)
    pieces, right, left = [block], block, block
    for _ in range((n - 1) // 2):
        right, left = shifted(right, axis, 1), shifted(left, axis, -1)
        pieces += [right, left]
    half = block.shape[0] // 2
    pieces.append(shifted(right[:half], axis, 1))
    pieces.append(shifted(left[half:], axis, -1))
    return pieces


def direct_pieces(block, axis):
    n = lax.axis_size(axis)
    return [block] + [shifted(block, axis, by) for by in sorted(range(1, n), key=lambda b: -min(b, n - b))]


def attention_kernel(n_kv, scale, q_ref, *refs):
    kv_refs = refs[:n_kv]
    o_ref, stat_ref, k0, k1, v, s_a, s_b, p_a, p_b = refs[n_kv:]
    ks = (k0, k1)
    at = 0
    for ref in kv_refs:
        n = ref.shape[0]
        k0[at : at + n] = ref[:, :128]
        k1[at : at + n] = ref[:, 128:256]
        v[at : at + n] = ref[:, 256:]
        at += n
    pieces, _, rows, _ = q_ref.shape
    sub = 16

    def score(i, m, s):
        s[...] = lax.dot_general(
            q_ref[i, m],
            ks[m][...],
            (((1,), (1,)), ((), ())),
            preferred_element_type=jnp.float32,
        )

    def soft(i, m, s, p):
        lane = lax.broadcasted_iota(jnp.int32, (sub, 128), 1)
        for r in range(0, rows, sub):
            x = s[r : r + sub]
            high = jnp.max(x, axis=1, keepdims=True)
            e = jnp.exp2((x - high) * (scale * LOG2E))
            p[r : r + sub] = e.astype(jnp.bfloat16)
            total = jnp.sum(e, axis=1, keepdims=True)
            stat_ref[i, m, r : r + sub] = jnp.where(lane == 0, high * scale, total)

    def mix(i, m, p):
        o = jnp.dot(p[...], v[...], preferred_element_type=jnp.float32)
        o_ref[i, m] = o.astype(o_ref.dtype)

    score(0, 0, s_a)

    def body(i, _):
        score(i, 1, s_b)

        @pl.when(i > 0)
        def _():
            mix(i - 1, 1, p_b)

        soft(i, 0, s_a, p_a)
        score(jnp.minimum(i + 1, pieces - 1), 0, s_a)
        mix(i, 0, p_a)
        soft(i, 1, s_b, p_b)
        return 0

    lax.fori_loop(0, pieces, body, 0)
    mix(pieces - 1, 1, p_b)


def attention(q, kvs, scale):
    pieces, _, rows, half = q.shape
    n_keys = sum(kv.shape[0] for kv in kvs)
    width = kvs[0].shape[1] - 2 * half
    vmem = pl.BlockSpec(memory_space=pltpu.VMEM)
    return pl.pallas_call(
        functools.partial(attention_kernel, len(kvs), scale),
        out_shape=(
            jax.ShapeDtypeStruct((pieces, 2, rows, width), jnp.bfloat16),
            jax.ShapeDtypeStruct((pieces, 2, rows, 128), jnp.float32),
        ),
        in_specs=[vmem] * (1 + len(kvs)),
        out_specs=(vmem, vmem),
        scratch_shapes=[pltpu.VMEM((n_keys, half), jnp.bfloat16)] * 2
        + [pltpu.VMEM((n_keys, width), jnp.bfloat16)]
        + [pltpu.VMEM((rows, n_keys), jnp.float32)] * 2
        + [pltpu.VMEM((rows, n_keys), jnp.bfloat16)] * 2,
        compiler_params=pltpu.CompilerParams(vmem_limit_bytes=48 * 1024 * 1024),
        name="attention",
    )(q, *kvs)


def merged(a, b):
    oa, ha, ta = a
    ob, hb, tb = b
    high = jnp.maximum(ha, hb)
    fa, fb = jnp.exp(ha - high), jnp.exp(hb - high)
    o = oa.astype(jnp.float32) * fa[..., None] + ob.astype(jnp.float32) * fb[..., None]
    return o, high, ta * fa + tb * fb


def swapped(part, axis):
    o, high, total = part
    perm = [(0, 1), (1, 0)]
    stats = lax.ppermute(jnp.stack([high, total]), axis, perm)
    return lax.ppermute(o.astype(jnp.bfloat16), axis, perm), stats[0], stats[1]


LANES = 128


def settle_kernel(parts, residual, gain, token, state, *refs):
    outs, normed, tiles = refs[:-2], refs[-2], refs[-1]
    rows, width = residual.shape
    high = width // LANES
    step = 16
    for r in range(0, rows, step):
        x = residual[r : r + step].astype(jnp.float32)
        share = parts[0, r : r + step].astype(jnp.float32)
        for p in range(1, parts.shape[0]):
            share = share + parts[p, r : r + step].astype(jnp.float32)
        x = x + share
        n = x * lax.rsqrt(jnp.mean(x * x, axis=1, keepdims=True) + EPS) * gain[...]
        for j in range(high):
            at = pl.ds(r * high + j, step, stride=high)
            state[at] = x[:, j * LANES : (j + 1) * LANES]
            normed[at] = n[:, j * LANES : (j + 1) * LANES]
    tiles[...] = normed[...].astype(jnp.bfloat16)
    places = outs[0].shape[0]
    for s, out in enumerate(outs):
        for e in range(places):
            t = pl.multiple_of(token[e * len(outs) + s] * high, high)
            out[e] = tiles[pl.ds(t, high)]


def settled(parts, residual, gain, token, places, slots):
    rows, width = residual.shape
    high = width // LANES
    vmem = pl.BlockSpec(memory_space=pltpu.VMEM)
    smem = pl.BlockSpec(memory_space=pltpu.SMEM)
    return pl.pallas_call(
        settle_kernel,
        out_shape=[jax.ShapeDtypeStruct((rows * high, LANES), jnp.float32)]
        + [jax.ShapeDtypeStruct((places, high, LANES), jnp.bfloat16)] * slots,
        in_specs=[vmem, vmem, vmem, smem],
        out_specs=[vmem] * (1 + slots),
        scratch_shapes=[
            pltpu.VMEM((rows * high, LANES), jnp.float32),
            pltpu.VMEM((rows * high, LANES), jnp.bfloat16),
        ],
        name="settle",
    )(parts, residual, gain, token)


def expert_kernel(count, *refs):
    blocks, (w_gate, w_up, w_down) = refs[:count], refs[count : count + 3]
    outs, (x, wide) = refs[count + 3 : 2 * count + 3], refs[2 * count + 3 :]
    high = blocks[0].shape[1]
    at = 0
    for block in blocks:
        n = block.shape[0]
        wide[: n * high] = block[...].reshape(n * high, LANES).astype(jnp.float32)
        for j in range(high):
            column = wide[pl.ds(j, n, stride=high)]
            x[at : at + n, j * LANES : (j + 1) * LANES] = column.astype(jnp.bfloat16)
        at += n
    gate = jnp.dot(x[...], w_gate[...], preferred_element_type=jnp.float32)
    up = jnp.dot(x[...], w_up[...], preferred_element_type=jnp.float32)
    hidden = (gate / (1.0 + jnp.exp(-gate)) * up).astype(jnp.bfloat16)
    result = jnp.dot(hidden, w_down[...], preferred_element_type=jnp.float32)
    at = 0
    for out in outs:
        n = out.shape[0]
        for j in range(high):
            wide[pl.ds(j, n, stride=high)] = result[at : at + n, j * LANES : (j + 1) * LANES]
        out[...] = wide[: n * high].astype(jnp.bfloat16).reshape(n, high, LANES)
        at += n


def expert(blocks, w_gate, w_up, w_down):
    total = sum(b.shape[0] for b in blocks)
    most = max(b.shape[0] for b in blocks)
    high = blocks[0].shape[1]
    vmem = pl.BlockSpec(memory_space=pltpu.VMEM)
    return pl.pallas_call(
        functools.partial(expert_kernel, len(blocks)),
        out_shape=[jax.ShapeDtypeStruct(b.shape, jnp.bfloat16) for b in blocks],
        in_specs=[vmem] * (len(blocks) + 3),
        out_specs=[vmem] * len(blocks),
        scratch_shapes=[
            pltpu.VMEM((total, high * LANES), jnp.bfloat16),
            pltpu.VMEM((most * high, LANES), jnp.float32),
        ],
        compiler_params=pltpu.CompilerParams(vmem_limit_bytes=40 * 1024 * 1024),
        name="expert",
    )(*blocks, w_gate, w_up, w_down)


def finish_kernel(slots, top, state, place, weight, *refs):
    returned, (out, wide) = refs[:slots], refs[slots:]
    rows, width = out.shape
    high = width // LANES
    for t in range(rows):
        y = state[t * high : (t + 1) * high]
        for r in range(top):
            k = t * top + r
            y = y + weight[k] * returned[0][place[k]].astype(jnp.float32)
        wide[t * high : (t + 1) * high] = y
    step = 16
    for r in range(0, rows, step):
        for j in range(high):
            column = wide[pl.ds(r * high + j, step, stride=high)]
            out[r : r + step, j * LANES : (j + 1) * LANES] = column.astype(jnp.bfloat16)


def finished(state, returned, place, weight, rows, top):
    high = returned.shape[1]
    vmem = pl.BlockSpec(memory_space=pltpu.VMEM)
    smem = pl.BlockSpec(memory_space=pltpu.SMEM)
    return pl.pallas_call(
        functools.partial(finish_kernel, 1, top),
        out_shape=jax.ShapeDtypeStruct((rows, high * LANES), jnp.bfloat16),
        in_specs=[vmem, smem, smem, vmem],
        out_specs=vmem,
        scratch_shapes=[pltpu.VMEM((rows * high, LANES), jnp.float32)],
        name="finish",
    )(state, place, weight, returned)


def copied_around(block):
    half = block.shape[0] // 2
    behind, ahead = shifted(block, TP, 1), shifted(block, TP, -1)
    return [
        block,
        behind,
        ahead,
        shifted(behind[:half], TP, 1),
        shifted(ahead[half:], TP, -1),
    ]


def summed_around(parts):
    own, behind, ahead, first, second = (p.astype(jnp.float32) for p in parts)
    half = parts[3].shape[0]
    first, second = shifted(parts[3], TP, 1), shifted(parts[4], TP, -1)
    zero = jnp.zeros(first.shape, jnp.float32)
    ahead = ahead + jnp.concatenate([first.astype(jnp.float32), zero])
    behind = behind + jnp.concatenate([zero, second.astype(jnp.float32)])
    from_behind = shifted(ahead.astype(jnp.bfloat16), TP, 1)
    from_ahead = shifted(behind.astype(jnp.bfloat16), TP, -1)
    total = own + from_behind.astype(jnp.float32) + from_ahead.astype(jnp.float32)
    return total.astype(jnp.bfloat16)


def exchanged(x):
    return lax.all_to_all(x, SP, split_axis=0, concat_axis=0, tiled=True)


def local(
    queries,
    keys,
    values,
    diff_scale,
    head_gain,
    w_out,
    residual,
    norm_gain,
    route_ids,
    route_weights,
    w_gate,
    w_up,
    w_down,
):
    q_rows = queries.shape[0]
    heads_dev = diff_scale.shape[0]
    half_dim = queries.shape[1] // (2 * heads_dev)
    group_cols = keys.shape[1] // KV_HEADS
    value_cols = values.shape[1] // KV_HEADS
    swap = [(0, 1), (1, 0)]

    group, quarter = lax.axis_index("xh"), lax.axis_index("xl")
    part_rows = q_rows // 2
    k_part = lax.dynamic_slice(
        keys, (quarter * part_rows, group * group_cols), (part_rows, group_cols)
    )
    v_part = lax.dynamic_slice(
        values, (quarter * part_rows, group * value_cols), (part_rows, value_cols)
    )
    joined = jnp.concatenate([k_part, v_part], axis=1)
    first, second = joined[: part_rows // 2], joined[part_rows // 2 :]
    q_own = queries.reshape(q_rows, heads_dev, 2, half_dim).transpose(2, 1, 0, 3)
    q_own = q_own.reshape(2, heads_dev * q_rows, half_dim)

    by_z = jnp.concatenate(direct_pieces(first, "y"))
    by_y = jnp.concatenate(direct_pieces(second, "z"))
    pieces = ring_pieces(by_z, "z") + ring_pieces(by_y, "y")
    q_core = lax.ppermute(q_own, "core", swap)
    q_x = lax.ppermute(q_own, "xl", swap)
    q_both = lax.ppermute(q_core, "xl", swap)

    o, stats = attention(
        jnp.stack([q_own, q_core, q_x, q_both]), pieces, 1.0 / math.sqrt(half_dim)
    )
    high, total = stats[..., 0], stats[..., 1]

    def part(i):
        return o[i], high[i], total[i]

    mine = merged(part(0), swapped(part(1), "core"))
    across = merged(part(2), swapped(part(3), "core"))
    acc, high, total = merged(mine, swapped(across, "xl"))

    acc = (acc / total[..., None]).reshape(2, heads_dev, q_rows, value_cols)
    mixed = acc[0] - diff_scale[:, None, None] * acc[1]
    mixed = mixed * lax.rsqrt(jnp.mean(mixed * mixed, axis=-1, keepdims=True) + EPS) * head_gain
    head_out = mixed.astype(jnp.bfloat16).transpose(1, 0, 2)
    head_out = head_out.reshape(q_rows, heads_dev * value_cols)
    rows_out = residual.shape[0]
    shares = jnp.dot(head_out, w_out, preferred_element_type=jnp.float32).astype(jnp.bfloat16)
    arrived = lax.all_to_all(
        cut_along(shares, 0, lax.axis_size(TP)), TP, split_axis=0, concat_axis=0, tiled=True
    )
    places = lax.axis_size(SP)
    top = route_ids.shape[1]
    slots = 2
    flat_ids = route_ids.reshape(-1)
    onehot = (flat_ids[:, None] == jnp.arange(places, dtype=jnp.int32)[None, :]).astype(jnp.int32)
    slot = jnp.sum((jnp.cumsum(onehot, axis=0) - onehot) * onehot, axis=1)
    dest = flat_ids * slots + slot
    taken = dest[:, None] == jnp.arange(places * slots, dtype=jnp.int32)[None, :]
    source = jnp.arange(flat_ids.shape[0], dtype=jnp.int32)[:, None] // top
    token = jnp.sum(jnp.where(taken, source, 0), axis=0)

    state, *outgoing = settled(arrived, residual, norm_gain[None, :], token, places, slots)
    outgoing = jnp.concatenate(outgoing, axis=1)
    high = outgoing.shape[1] // slots
    received = exchanged(outgoing).reshape(places * slots, high, LANES)
    parts = expert(copied_around(received), w_gate[0], w_up[0], w_down[0])
    back = summed_around(parts).reshape(places, slots * high, LANES)
    returned = exchanged(back).reshape(places * slots, high, LANES)
    place = dest
    return finished(state, returned, place, route_weights.reshape(-1), rows_out, top)


def solution(mesh):
    cells = mesh.devices.reshape(8, 4, 2, 2, 2)
    mesh = Mesh(cells, ("z", "y", "core", "xh", "xl"))
    in_specs = (
        P(SP, TP),
        P(SP, None),
        P(SP, None),
        P(TP),
        P(),
        P(TP, None),
        P(SP + TP, None),
        P(),
        P(SP + TP, None),
        P(SP + TP, None),
        P(SP, None, TP),
        P(SP, None, TP),
        P(SP, TP, None),
    )
    out_specs = P(SP + TP, None)
    return jax.shard_map(local, mesh=mesh, in_specs=in_specs, out_specs=out_specs, check_vma=False)
```

```python
import functools
import math

import jax
import jax.numpy as jnp
from jax import lax
from jax.experimental import pallas as pl
from jax.experimental.pallas import tpu as pltpu
from jax.sharding import Mesh
from jax.sharding import PartitionSpec as P

KV_HEADS = 2
SP = ("z", "y", "core")
TP = ("xh", "xl")


EPS = 1e-06
LOG2E = math.log2(math.e)


def cut_along(shard, dim, peers):
    before, after = (shard.shape[:dim], shard.shape[dim + 1 :])
    return jnp.moveaxis(shard.reshape(*before, peers, -1, *after), dim, 0)


def shifted(x, axis, by):
    n = lax.axis_size(axis)
    return lax.ppermute(x, axis, [(i, (i + by) % n) for i in range(n)])


def attention_kernel(n_q, n_kv, first, last, scale, *refs):
    q_refs, kv_refs = refs[:n_q], refs[n_q : n_q + n_kv]
    refs = refs[n_q + n_kv :]
    if not first:
        acc_in, high_in, total_in, *refs = refs
    if last:
        kept, sent, kept_stat, sent_stat, *refs = refs
    else:
        acc, high, total, *refs = refs
    q, k0, k1, v, s_a, s_b, p_a, p_b, f_a, f_b, h_a, h_b, t_a, t_b = refs
    ks = (k0, k1)
    at = 0
    for ref in kv_refs:
        n = ref.shape[0]
        k0[at : at + n] = ref[:, :128]
        k1[at : at + n] = ref[:, 128:256]
        v[at : at + n] = ref[:, 256:]
        at += n
    for i, ref in enumerate(q_refs):
        q[i] = ref[...]
    pieces, _, rows, _ = q.shape
    sub = 16
    c = scale * LOG2E
    keep = pieces // 2

    def score(i, m, s):
        s[...] = lax.dot_general(
            q[i, m], ks[m][...], (((1,), (1,)), ((), ())), preferred_element_type=jnp.float32
        )

    def soft(i, m, s, p, f, h, t, stat):
        lane = lax.broadcasted_iota(jnp.int32, (sub, 128), 1)
        n = s.shape[1] // 128
        if not first:
            h[0] = high_in[i, m]
            t[0] = total_in[i, m]
        for r in range(0, rows, sub):
            part = slice(r, r + sub)
            x = [s[part, g * 128 : (g + 1) * 128] for g in range(n)]
            top = jnp.max(functools.reduce(jnp.maximum, x), axis=1, keepdims=True)
            peak = jnp.broadcast_to(top, (sub, 128))
            if not first:
                before = h[0, part]
                peak = jnp.maximum(before, peak)
                fade = jnp.exp2((before - peak) * c)
                f[part] = fade
            e = [jnp.exp2((y - peak) * c) for y in x]
            for g in range(n):
                p[part, g * 128 : (g + 1) * 128] = e[g].astype(jnp.bfloat16)
            count = jnp.sum(functools.reduce(jnp.add, e), axis=1, keepdims=True)
            count = jnp.broadcast_to(count, (sub, 128))
            if not first:
                count = count + t[0, part] * fade
            if last:
                h[1, part] = jnp.where(lane == 0, peak * scale, count)
            else:
                h[1, part] = peak
                t[1, part] = count
        if last:
            stat[i % keep * 2 + m] = jnp.transpose(h[1])[:8]
        else:
            high[i, m] = h[1]
            total[i, m] = t[1]

    def mix(i, m, p, f, out):
        o = jnp.dot(p[...], v[...], preferred_element_type=jnp.float32)
        at = i % keep if last else i
        for g in range(0, o.shape[1], 128):
            part = o[:, g : g + 128]
            if not first:
                part = part + acc_in[i, m, :, g : g + 128] * f[...]
            out[at, m, :, g : g + 128] = part.astype(out.dtype)

    def run(start, stop, out, stat):
        score(start, 0, s_a)

        def body(i, _):
            score(i, 1, s_b)

            @pl.when(i > start)
            def _():
                mix(i - 1, 1, p_b, f_b, out)

            soft(i, 0, s_a, p_a, f_a, h_a, t_a, stat)
            score(jnp.minimum(i + 1, stop - 1), 0, s_a)
            mix(i, 0, p_a, f_a, out)
            soft(i, 1, s_b, p_b, f_b, h_b, t_b, stat)
            return 0

        lax.fori_loop(start, stop, body, 0)
        mix(stop - 1, 1, p_b, f_b, out)

    if last:
        run(keep, pieces, sent, sent_stat)
        run(0, keep, kept, kept_stat)
    else:
        run(0, pieces, acc, None)


def attention(qs, kvs, carry, last, scale):
    pieces = len(qs)
    _, rows, half = qs[0].shape
    n_keys = sum(kv.shape[0] for kv in kvs)
    width = kvs[0].shape[1] - 2 * half
    vmem = pl.BlockSpec(memory_space=pltpu.VMEM)
    keep = pieces // 2
    if last:
        out_shape = [
            jax.ShapeDtypeStruct((keep, 2, rows, width), jnp.float32),
            jax.ShapeDtypeStruct((keep, 2, rows, width), jnp.bfloat16),
            jax.ShapeDtypeStruct((2 * keep, 8, rows), jnp.float32),
            jax.ShapeDtypeStruct((2 * keep, 8, rows), jnp.float32),
        ]
    else:
        out_shape = [
            jax.ShapeDtypeStruct((pieces, 2, rows, width), jnp.float32),
            jax.ShapeDtypeStruct((pieces, 2, rows, 128), jnp.float32),
            jax.ShapeDtypeStruct((pieces, 2, rows, 128), jnp.float32),
        ]
    n_in = pieces + len(kvs)
    aliases = {n_in + i: i for i in range(3)} if carry and not last else {}
    return pl.pallas_call(
        functools.partial(attention_kernel, pieces, len(kvs), not carry, last, scale),
        out_shape=out_shape,
        in_specs=[vmem] * (n_in + len(carry)),
        out_specs=[vmem] * len(out_shape),
        scratch_shapes=[pltpu.VMEM((pieces, 2, rows, half), jnp.bfloat16)]
        + [pltpu.VMEM((n_keys, half), jnp.bfloat16)] * 2
        + [pltpu.VMEM((n_keys, width), jnp.bfloat16)]
        + [pltpu.VMEM((rows, n_keys), jnp.float32)] * 2
        + [pltpu.VMEM((rows, n_keys), jnp.bfloat16)] * 2
        + [pltpu.VMEM((rows, 128), jnp.float32)] * 2
        + [pltpu.VMEM((2, rows, 128), jnp.float32)] * 4,
        input_output_aliases=aliases,
        compiler_params=pltpu.CompilerParams(vmem_limit_bytes=32 * 1024 * 1024),
        cost_estimate=pl.CostEstimate(
            flops=4 * pieces * rows * n_keys * (half + width),
            bytes_accessed=n_keys * (2 * half + width) * 2,
            transcendentals=2 * pieces * rows * n_keys,
        ),
        name="attention",
    )(*qs, *kvs, *carry)


def factors(stat_a, stat_b):
    high = jnp.maximum(stat_a[0:1], stat_b[0:1])
    fade_a, fade_b = jnp.exp(stat_a[0:1] - high), jnp.exp(stat_b[0:1] - high)
    return fade_a, fade_b, high, stat_a[1:2] * fade_a + stat_b[1:2] * fade_b


def scaled_sum(a, factor_a, b, factor_b):
    rows = a.shape[0]
    fa = jnp.transpose(jnp.broadcast_to(factor_a, (128, rows)))
    fb = jnp.transpose(jnp.broadcast_to(factor_b, (128, rows)))
    parts = []
    for g in range(0, a.shape[1], 128):
        part = slice(g, g + 128)
        parts.append(a[:, part] * fa + b[:, part].astype(jnp.float32) * fb)
    return parts


def core_merge_kernel(kept, kept_stat, came, came_stat, own, own_stat, across, across_stat):
    rows = own.shape[1]
    line = lax.broadcasted_iota(jnp.int32, (8, rows), 0)
    for i, (out, stat) in enumerate(((own, own_stat), (across, across_stat))):
        for m in range(2):
            at = 2 * i + m
            fa, fb, high, total = factors(kept_stat[at], came_stat[at])
            parts = scaled_sum(kept[i, m], fa, came[i, m], fb)
            for g, part in enumerate(parts):
                out[m, :, g * 128 : (g + 1) * 128] = part.astype(out.dtype)
            stat[m] = jnp.where(line == 0, high, total)


def core_merged(kept, kept_stat, came, came_stat):
    _, _, rows, width = kept.shape
    vmem = pl.BlockSpec(memory_space=pltpu.VMEM)
    stat = jax.ShapeDtypeStruct((2, 8, rows), jnp.float32)
    return pl.pallas_call(
        core_merge_kernel,
        out_shape=[
            jax.ShapeDtypeStruct((2, rows, width), jnp.float32),
            stat,
            jax.ShapeDtypeStruct((2, rows, width), jnp.bfloat16),
            stat,
        ],
        in_specs=[vmem] * 4,
        out_specs=[vmem] * 4,
        compiler_params=pltpu.CompilerParams(vmem_limit_bytes=8 * 1024 * 1024),
        name="core_merge",
    )(kept, kept_stat, came, came_stat)


def project_kernel(own, own_stat, came, came_stat, diff_scale, gain, w_out, shares, head_out):
    rows, heads = shares.shape[0], diff_scale.shape[0]
    width = own.shape[2]
    maps = []
    for m in range(2):
        fa, fb, _, total = factors(own_stat[m], came_stat[m])
        maps.append(scaled_sum(own[m], fa / total, came[m], fb / total))
    for h in range(heads):
        part = slice(h * rows, (h + 1) * rows)
        mixed = [a[part] - diff_scale[h] * b[part] for a, b in zip(*maps)]
        mean = sum(jnp.sum(x * x, axis=1, keepdims=True) for x in mixed) / width
        norm = lax.rsqrt(mean + EPS)
        for g, x in enumerate(mixed):
            at = slice(h * width + g * 128, h * width + (g + 1) * 128)
            x = x * norm * gain[:, g * 128 : (g + 1) * 128]
            head_out[:, at] = x.astype(jnp.bfloat16)
    out = jnp.dot(head_out[...], w_out[...], preferred_element_type=jnp.float32)
    shares[...] = out.astype(jnp.bfloat16)


def projected(own, own_stat, came, came_stat, diff_scale, gain, w_out, rows):
    vmem = pl.BlockSpec(memory_space=pltpu.VMEM)
    smem = pl.BlockSpec(memory_space=pltpu.SMEM)
    return pl.pallas_call(
        project_kernel,
        out_shape=jax.ShapeDtypeStruct((rows, w_out.shape[1]), jnp.bfloat16),
        in_specs=[vmem] * 4 + [smem, vmem, vmem],
        out_specs=vmem,
        scratch_shapes=[pltpu.VMEM((rows, w_out.shape[0]), jnp.bfloat16)],
        compiler_params=pltpu.CompilerParams(vmem_limit_bytes=12 * 1024 * 1024),
        name="project",
    )(own, own_stat, came, came_stat, diff_scale, gain, w_out)


LANES = 128


def settle_kernel(parts, residual, gain, token, state, *refs):
    outs, normed, tiles = refs[:-2], refs[-2], refs[-1]
    rows, width = residual.shape
    high = width // LANES
    step = 16
    for r in range(0, rows, step):
        x = residual[r : r + step].astype(jnp.float32)
        share = parts[0, r : r + step].astype(jnp.float32)
        for p in range(1, parts.shape[0]):
            share = share + parts[p, r : r + step].astype(jnp.float32)
        x = x + share
        n = x * lax.rsqrt(jnp.mean(x * x, axis=1, keepdims=True) + EPS) * gain[...]
        for j in range(high):
            at = pl.ds(r * high + j, step, stride=high)
            state[at] = x[:, j * LANES : (j + 1) * LANES]
            normed[at] = n[:, j * LANES : (j + 1) * LANES]
    tiles[...] = normed[...].astype(jnp.bfloat16)
    places = outs[0].shape[0]
    for s, out in enumerate(outs):
        for e in range(places):
            t = pl.multiple_of(token[e * len(outs) + s] * high, high)
            out[e] = tiles[pl.ds(t, high)]


def settled(parts, residual, gain, token, places, slots):
    rows, width = residual.shape
    high = width // LANES
    vmem = pl.BlockSpec(memory_space=pltpu.VMEM)
    smem = pl.BlockSpec(memory_space=pltpu.SMEM)
    return pl.pallas_call(
        settle_kernel,
        out_shape=[jax.ShapeDtypeStruct((rows * high, LANES), jnp.float32)]
        + [jax.ShapeDtypeStruct((places, high, LANES), jnp.bfloat16)] * slots,
        in_specs=[vmem, vmem, vmem, smem],
        out_specs=[vmem] * (1 + slots),
        scratch_shapes=[
            pltpu.VMEM((rows * high, LANES), jnp.float32),
            pltpu.VMEM((rows * high, LANES), jnp.bfloat16),
        ],
        compiler_params=pltpu.CompilerParams(vmem_limit_bytes=6 * 1024 * 1024),
        name="settle",
    )(parts, residual, gain, token)


def expert_kernel(count, *refs):
    blocks, (w_gate, w_up, w_down) = refs[:count], refs[count : count + 3]
    outs, (x, wide) = refs[count + 3 : 2 * count + 3], refs[2 * count + 3 :]
    high = blocks[0].shape[1]
    at = 0
    for block in blocks:
        n = block.shape[0]
        wide[: n * high] = block[...].reshape(n * high, LANES).astype(jnp.float32)
        for j in range(high):
            column = wide[pl.ds(j, n, stride=high)]
            x[at : at + n, j * LANES : (j + 1) * LANES] = column.astype(jnp.bfloat16)
        at += n
    gate = jnp.dot(x[...], w_gate[...], preferred_element_type=jnp.float32)
    up = jnp.dot(x[...], w_up[...], preferred_element_type=jnp.float32)
    hidden = (gate / (1.0 + jnp.exp(-gate)) * up).astype(jnp.bfloat16)
    result = jnp.dot(hidden, w_down[...], preferred_element_type=jnp.float32)
    at = 0
    for out in outs:
        n = out.shape[0]
        for j in range(high):
            wide[pl.ds(j, n, stride=high)] = result[at : at + n, j * LANES : (j + 1) * LANES]
        out[...] = wide[: n * high].astype(jnp.bfloat16).reshape(n, high, LANES)
        at += n


def expert(blocks, w_gate, w_up, w_down):
    total = sum(b.shape[0] for b in blocks)
    most = max(b.shape[0] for b in blocks)
    high = blocks[0].shape[1]
    vmem = pl.BlockSpec(memory_space=pltpu.VMEM)
    return pl.pallas_call(
        functools.partial(expert_kernel, len(blocks)),
        out_shape=[jax.ShapeDtypeStruct(b.shape, jnp.bfloat16) for b in blocks],
        in_specs=[vmem] * (len(blocks) + 3),
        out_specs=[vmem] * len(blocks),
        scratch_shapes=[
            pltpu.VMEM((total, high * LANES), jnp.bfloat16),
            pltpu.VMEM((most * high, LANES), jnp.float32),
        ],
        compiler_params=pltpu.CompilerParams(vmem_limit_bytes=24 * 1024 * 1024),
        name="expert",
    )(*blocks, w_gate, w_up, w_down)


def finish_kernel(slots, top, state, place, weight, *refs):
    returned, (out, wide) = refs[:slots], refs[slots:]
    rows, width = out.shape
    high = width // LANES
    for t in range(rows):
        y = state[t * high : (t + 1) * high]
        for r in range(top):
            k = t * top + r
            y = y + weight[k] * returned[0][place[k]].astype(jnp.float32)
        wide[t * high : (t + 1) * high] = y
    step = 16
    for r in range(0, rows, step):
        for j in range(high):
            column = wide[pl.ds(r * high + j, step, stride=high)]
            out[r : r + step, j * LANES : (j + 1) * LANES] = column.astype(jnp.bfloat16)


def finished(state, returned, place, weight, rows, top):
    high = returned.shape[1]
    vmem = pl.BlockSpec(memory_space=pltpu.VMEM)
    smem = pl.BlockSpec(memory_space=pltpu.SMEM)
    return pl.pallas_call(
        functools.partial(finish_kernel, 1, top),
        out_shape=jax.ShapeDtypeStruct((rows, high * LANES), jnp.bfloat16),
        in_specs=[vmem, smem, smem, vmem],
        out_specs=vmem,
        scratch_shapes=[pltpu.VMEM((rows * high, LANES), jnp.float32)],
        compiler_params=pltpu.CompilerParams(vmem_limit_bytes=6 * 1024 * 1024),
        name="finish",
    )(state, place, weight, returned)


def copied_around(block):
    half = block.shape[0] // 2
    behind, ahead = shifted(block, TP, 1), shifted(block, TP, -1)
    return [
        block,
        behind,
        ahead,
        shifted(behind[:half], TP, 1),
        shifted(ahead[half:], TP, -1),
    ]


def summed_around(parts):
    own, behind, ahead, first, second = (p.astype(jnp.float32) for p in parts)
    half = parts[3].shape[0]
    first, second = shifted(parts[3], TP, 1), shifted(parts[4], TP, -1)
    zero = jnp.zeros(first.shape, jnp.float32)
    ahead = ahead + jnp.concatenate([first.astype(jnp.float32), zero])
    behind = behind + jnp.concatenate([zero, second.astype(jnp.float32)])
    from_behind = shifted(ahead.astype(jnp.bfloat16), TP, 1)
    from_ahead = shifted(behind.astype(jnp.bfloat16), TP, -1)
    total = own + from_behind.astype(jnp.float32) + from_ahead.astype(jnp.float32)
    return total.astype(jnp.bfloat16)


def exchanged(x):
    return lax.all_to_all(x, SP, split_axis=0, concat_axis=0, tiled=True)


def local(
    queries,
    keys,
    values,
    diff_scale,
    head_gain,
    w_out,
    residual,
    norm_gain,
    route_ids,
    route_weights,
    w_gate,
    w_up,
    w_down,
):
    q_rows = queries.shape[0]
    heads_dev = diff_scale.shape[0]
    half_dim = queries.shape[1] // (2 * heads_dev)
    group_cols = keys.shape[1] // KV_HEADS
    value_cols = values.shape[1] // KV_HEADS
    swap = [(0, 1), (1, 0)]

    group, quarter = lax.axis_index("xh"), lax.axis_index("xl")
    part_rows = q_rows // 2
    k_part = lax.dynamic_slice(
        keys, (quarter * part_rows, group * group_cols), (part_rows, group_cols)
    )
    v_part = lax.dynamic_slice(
        values, (quarter * part_rows, group * value_cols), (part_rows, value_cols)
    )
    joined = jnp.concatenate([k_part, v_part], axis=1)
    q_own = jnp.stack(
        [
            jnp.concatenate(
                [
                    queries[:, (2 * h + m) * half_dim : (2 * h + m + 1) * half_dim]
                    for h in range(heads_dev)
                ]
            )
            for m in range(2)
        ]
    )

    sides = [joined] + [shifted(joined, "y", by) for by in (1, -1, 2)]
    q_core = lax.ppermute(q_own, "core", swap)
    q_x = lax.ppermute(q_own, "xl", swap)
    q_both = lax.ppermute(q_x, "core", swap)
    block, q_core, q_x = lax.optimization_barrier((jnp.concatenate(sides), q_core, q_x))
    qs = [q_own, q_x, q_core, q_both]
    scale = 1.0 / math.sqrt(half_dim)
    n = lax.axis_size("z")
    right, left = shifted(block, "z", 1), shifted(block, "z", -1)
    kvs, carry = [block, right, left], []
    for step in range(2, n // 2 + 1):
        if step == n // 2:
            half = block.shape[0] // 2
            right, left = right[:half], left[half:]
        right, left = shifted(right, "z", 1), shifted(left, "z", -1)
        carry = attention(qs, kvs, carry, False, scale)
        right, left, *carry = lax.optimization_barrier((right, left, *carry))
        kvs = [right, left]
    carry = attention(qs, kvs, carry, True, scale)
    kept, sent, kept_stat, sent_stat = carry
    came = [lax.ppermute(x, "core", swap) for x in (sent, sent_stat)]
    own, own_stat, across, across_stat = core_merged(kept, kept_stat, *came)
    came = [lax.ppermute(x, "xl", swap) for x in (across, across_stat)]
    shares = projected(own, own_stat, *came, diff_scale, head_gain[None, :], w_out, q_rows)
    rows_out = residual.shape[0]
    arrived = lax.all_to_all(
        cut_along(shares, 0, lax.axis_size(TP)), TP, split_axis=0, concat_axis=0, tiled=True
    )
    places = lax.axis_size(SP)
    top = route_ids.shape[1]
    slots = 2
    flat_ids = route_ids.reshape(-1)
    onehot = (flat_ids[:, None] == jnp.arange(places, dtype=jnp.int32)[None, :]).astype(jnp.int32)
    slot = jnp.sum((jnp.cumsum(onehot, axis=0) - onehot) * onehot, axis=1)
    dest = flat_ids * slots + slot
    taken = dest[:, None] == jnp.arange(places * slots, dtype=jnp.int32)[None, :]
    source = jnp.arange(flat_ids.shape[0], dtype=jnp.int32)[:, None] // top
    token = jnp.sum(jnp.where(taken, source, 0), axis=0)

    state, *outgoing = settled(arrived, residual, norm_gain[None, :], token, places, slots)
    outgoing = jnp.concatenate(outgoing, axis=1)
    high = outgoing.shape[1] // slots
    received = exchanged(outgoing).reshape(places * slots, high, LANES)
    parts = expert(copied_around(received), w_gate[0], w_up[0], w_down[0])
    back = summed_around(parts).reshape(places, slots * high, LANES)
    returned = exchanged(back).reshape(places * slots, high, LANES)
    place = dest
    return finished(state, returned, place, route_weights.reshape(-1), rows_out, top)


def solution(mesh):
    cells = mesh.devices.reshape(8, 4, 2, 2, 2)
    mesh = Mesh(cells, ("z", "y", "core", "xh", "xl"))
    in_specs = (
        P(SP, TP),
        P(SP, None),
        P(SP, None),
        P(TP),
        P(),
        P(TP, None),
        P(SP + TP, None),
        P(),
        P(SP + TP, None),
        P(SP + TP, None),
        P(SP, None, TP),
        P(SP, None, TP),
        P(SP, TP, None),
    )
    out_specs = P(SP + TP, None)
    return jax.shard_map(local, mesh=mesh, in_specs=in_specs, out_specs=out_specs, check_vma=False)
```

```python
import functools
import math

import jax
import jax.numpy as jnp
from jax import lax
from jax.experimental import pallas as pl
from jax.experimental.pallas import tpu as pltpu
from jax.sharding import Mesh
from jax.sharding import PartitionSpec as P

KV_HEADS = 2
SP = ("z", "y", "core")
TP = ("xh", "xl")


EPS = 1e-06
LOG2E = math.log2(math.e)


def cut_along(shard, dim, peers):
    before, after = (shard.shape[:dim], shard.shape[dim + 1 :])
    return jnp.moveaxis(shard.reshape(*before, peers, -1, *after), dim, 0)


def shifted(x, axis, by):
    n = lax.axis_size(axis)
    return lax.ppermute(x, axis, [(i, (i + by) % n) for i in range(n)])


STAT_ROWS = 16


def stats_block(high, total):
    line = lax.broadcasted_iota(jnp.int32, (STAT_ROWS, 256), 0)
    block = jnp.zeros((STAT_ROWS, 256), jnp.float32)
    for i, row in enumerate((high, total)):
        for k in range(3):
            part = row.astype(jnp.bfloat16).astype(jnp.float32)
            row = row - part
            tail = jnp.concatenate([part[:, 256:], part[:, 256:]], axis=1)
            block = jnp.where(line == 3 * i + k, part[:, :256], block)
            block = jnp.where(line == 6 + 3 * i + k, tail, block)
    return block.astype(jnp.bfloat16)


def stats_rows(block):
    block = block.astype(jnp.float32)
    rows = []
    for i in range(2):
        first, tail = (
            block[at : at + 1] + block[at + 1 : at + 2] + block[at + 2 : at + 3]
            for at in (3 * i, 6 + 3 * i)
        )
        rows.append(jnp.concatenate([first, tail[:, :128]], axis=1))
    return rows


def attention_kernel(n_q, n_kv, first, last, scale, *refs):
    q_refs, kv_refs = refs[:n_q], refs[n_q : n_q + n_kv]
    refs = refs[n_q + n_kv :]
    if not first:
        acc_in, high_in, total_in, *refs = refs
    if last:
        kept, sent, kept_stat, *refs = refs
    else:
        acc, high, total, *refs = refs
    q, k0, k1, v, s_a, s_b, p_a, p_b, f_a, f_b, h_a, h_b, t_a, t_b = refs
    ks = (k0, k1)
    at = 0
    for ref in kv_refs:
        n = ref.shape[0]
        k0[at : at + n] = ref[:, :128]
        k1[at : at + n] = ref[:, 128:256]
        v[at : at + n] = ref[:, 256:]
        at += n
    for i, ref in enumerate(q_refs):
        q[2 * i : 2 * i + 2] = ref[...]
    pieces, _, rows, _ = q.shape
    sub = 16
    c = scale * LOG2E
    keep = pieces // 2

    def score(i, m, s):
        s[...] = lax.dot_general(
            q[i, m], ks[m][...], (((1,), (1,)), ((), ())), preferred_element_type=jnp.float32
        )

    def soft(i, m, s, p, f, h, t, stat):
        lane = lax.broadcasted_iota(jnp.int32, (sub, 128), 1)
        n = s.shape[1] // 128
        if not first:
            h[0] = high_in[i, m]
            t[0] = total_in[i, m]
        for r in range(0, rows, sub):
            part = slice(r, r + sub)
            x = [s[part, g * 128 : (g + 1) * 128] for g in range(n)]
            top = jnp.max(functools.reduce(jnp.maximum, x), axis=1, keepdims=True)
            peak = jnp.broadcast_to(top, (sub, 128))
            if not first:
                before = h[0, part]
                peak = jnp.maximum(before, peak)
                fade = jnp.exp2((before - peak) * c)
                f[part] = fade
            e = [jnp.exp2((y - peak) * c) for y in x]
            for g in range(n):
                p[part, g * 128 : (g + 1) * 128] = e[g].astype(jnp.bfloat16)
            count = jnp.sum(functools.reduce(jnp.add, e), axis=1, keepdims=True)
            count = jnp.broadcast_to(count, (sub, 128))
            if not first:
                count = count + t[0, part] * fade
            if last:
                h[1, part] = jnp.where(lane == 0, peak * scale, count)
            else:
                h[1, part] = peak
                t[1, part] = count
        if last:
            turned = jnp.transpose(h[1])
            if stat is None:
                sent[i % keep, m, rows:] = stats_block(turned[0:1], turned[1:2])
            else:
                stat[i * 2 + m] = turned[:8]
        else:
            high[i, m] = h[1]
            total[i, m] = t[1]

    def mix(i, m, p, f, out):
        o = jnp.dot(p[...], v[...], preferred_element_type=jnp.float32)
        at = i % keep if last else i
        for g in range(0, o.shape[1], 128):
            part = o[:, g : g + 128]
            if not first:
                part = part + acc_in[i, m, :, g : g + 128] * f[...]
            out[at, m, :rows, g : g + 128] = part.astype(out.dtype)

    def run(start, stop, out, stat):
        score(start, 0, s_a)

        def body(i, _):
            score(i, 1, s_b)

            @pl.when(i > start)
            def _():
                mix(i - 1, 1, p_b, f_b, out)

            soft(i, 0, s_a, p_a, f_a, h_a, t_a, stat)
            score(jnp.minimum(i + 1, stop - 1), 0, s_a)
            mix(i, 0, p_a, f_a, out)
            soft(i, 1, s_b, p_b, f_b, h_b, t_b, stat)
            return 0

        lax.fori_loop(start, stop, body, 0)
        mix(stop - 1, 1, p_b, f_b, out)

    if last:
        run(keep, pieces, sent, None)
        run(0, keep, kept, kept_stat)
    else:
        run(0, pieces, acc, None)


def attention(qs, kvs, carry, last, scale):
    pieces = 2 * len(qs)
    _, _, rows, half = qs[0].shape
    n_keys = sum(kv.shape[0] for kv in kvs)
    width = kvs[0].shape[1] - 2 * half
    vmem = pl.BlockSpec(memory_space=pltpu.VMEM)
    keep = pieces // 2
    if last:
        out_shape = [
            jax.ShapeDtypeStruct((keep, 2, rows, width), jnp.float32),
            jax.ShapeDtypeStruct((keep, 2, rows + STAT_ROWS, width), jnp.bfloat16),
            jax.ShapeDtypeStruct((2 * keep, 8, rows), jnp.float32),
        ]
    else:
        out_shape = [
            jax.ShapeDtypeStruct((pieces, 2, rows, width), jnp.float32),
            jax.ShapeDtypeStruct((pieces, 2, rows, 128), jnp.float32),
            jax.ShapeDtypeStruct((pieces, 2, rows, 128), jnp.float32),
        ]
    n_in = len(qs) + len(kvs)
    aliases = {n_in + i: i for i in range(3)} if carry and not last else {}
    return pl.pallas_call(
        functools.partial(attention_kernel, len(qs), len(kvs), not carry, last, scale),
        out_shape=out_shape,
        in_specs=[vmem] * (n_in + len(carry)),
        out_specs=[vmem] * len(out_shape),
        scratch_shapes=[pltpu.VMEM((pieces, 2, rows, half), jnp.bfloat16)]
        + [pltpu.VMEM((n_keys, half), jnp.bfloat16)] * 2
        + [pltpu.VMEM((n_keys, width), jnp.bfloat16)]
        + [pltpu.VMEM((rows, n_keys), jnp.float32)] * 2
        + [pltpu.VMEM((rows, n_keys), jnp.bfloat16)] * 2
        + [pltpu.VMEM((rows, 128), jnp.float32)] * 2
        + [pltpu.VMEM((2, rows, 128), jnp.float32)] * 4,
        input_output_aliases=aliases,
        compiler_params=pltpu.CompilerParams(vmem_limit_bytes=32 * 1024 * 1024),
        cost_estimate=pl.CostEstimate(
            flops=4 * pieces * rows * n_keys * (half + width),
            bytes_accessed=n_keys * (2 * half + width) * 2,
            transcendentals=2 * pieces * rows * n_keys,
        ),
        name="attention",
    )(*qs, *kvs, *carry)


def factors(high_a, total_a, high_b, total_b):
    high = jnp.maximum(high_a, high_b)
    fade_a, fade_b = jnp.exp(high_a - high), jnp.exp(high_b - high)
    return fade_a, fade_b, high, total_a * fade_a + total_b * fade_b


def scaled_sum(a, factor_a, b, factor_b):
    rows = a.shape[0]
    fa = jnp.transpose(jnp.broadcast_to(factor_a, (128, rows)))
    fb = jnp.transpose(jnp.broadcast_to(factor_b, (128, rows)))
    parts = []
    for g in range(0, a.shape[1], 128):
        part = slice(g, g + 128)
        parts.append(a[:, part] * fa + b[:, part].astype(jnp.float32) * fb)
    return parts


def core_merge_kernel(kept, kept_stat, came, own, own_stat, across):
    rows = own.shape[1]
    line = lax.broadcasted_iota(jnp.int32, (8, rows), 0)
    for i, out in enumerate((own, across)):
        for m in range(2):
            at = 2 * i + m
            stats = stats_rows(came[i, m, rows:])
            fa, fb, high, total = factors(kept_stat[at, 0:1], kept_stat[at, 1:2], *stats)
            parts = scaled_sum(kept[i, m], fa, came[i, m, :rows], fb)
            for g, part in enumerate(parts):
                out[m, :rows, g * 128 : (g + 1) * 128] = part.astype(out.dtype)
            if i == 0:
                own_stat[m] = jnp.where(line == 0, high, total)
            else:
                across[m, rows:] = stats_block(high, total)


def core_merged(kept, kept_stat, came):
    _, _, rows, width = kept.shape
    vmem = pl.BlockSpec(memory_space=pltpu.VMEM)
    return pl.pallas_call(
        core_merge_kernel,
        out_shape=[
            jax.ShapeDtypeStruct((2, rows, width), jnp.float32),
            jax.ShapeDtypeStruct((2, 8, rows), jnp.float32),
            jax.ShapeDtypeStruct((2, rows + STAT_ROWS, width), jnp.bfloat16),
        ],
        in_specs=[vmem] * 3,
        out_specs=[vmem] * 3,
        compiler_params=pltpu.CompilerParams(vmem_limit_bytes=8 * 1024 * 1024),
        name="core_merge",
    )(kept, kept_stat, came)


def project_kernel(own, own_stat, came, diff_scale, gain, w_out, shares, head_out):
    rows, heads = shares.shape[0], diff_scale.shape[0]
    width = own.shape[2]
    maps = []
    for m in range(2):
        each = own.shape[1]
        stats = stats_rows(came[m, each:])
        fa, fb, _, total = factors(own_stat[m, 0:1], own_stat[m, 1:2], *stats)
        maps.append(scaled_sum(own[m], fa / total, came[m, :each], fb / total))
    for h in range(heads):
        part = slice(h * rows, (h + 1) * rows)
        mixed = [a[part] - diff_scale[h] * b[part] for a, b in zip(*maps)]
        mean = sum(jnp.sum(x * x, axis=1, keepdims=True) for x in mixed) / width
        norm = lax.rsqrt(mean + EPS)
        for g, x in enumerate(mixed):
            at = slice(h * width + g * 128, h * width + (g + 1) * 128)
            x = x * norm * gain[:, g * 128 : (g + 1) * 128]
            head_out[:, at] = x.astype(jnp.bfloat16)
    out = jnp.dot(head_out[...], w_out[...], preferred_element_type=jnp.float32)
    shares[...] = out.astype(jnp.bfloat16)


def projected(own, own_stat, came, diff_scale, gain, w_out, rows):
    vmem = pl.BlockSpec(memory_space=pltpu.VMEM)
    smem = pl.BlockSpec(memory_space=pltpu.SMEM)
    return pl.pallas_call(
        project_kernel,
        out_shape=jax.ShapeDtypeStruct((rows, w_out.shape[1]), jnp.bfloat16),
        in_specs=[vmem] * 3 + [smem, vmem, vmem],
        out_specs=vmem,
        scratch_shapes=[pltpu.VMEM((rows, w_out.shape[0]), jnp.bfloat16)],
        compiler_params=pltpu.CompilerParams(vmem_limit_bytes=12 * 1024 * 1024),
        name="project",
    )(own, own_stat, came, diff_scale, gain, w_out)


LANES = 128


def settle_kernel(parts, residual, gain, token, state, *refs):
    outs, normed, tiles = refs[:-2], refs[-2], refs[-1]
    rows, width = residual.shape
    high = width // LANES
    step = 16
    for r in range(0, rows, step):
        x = residual[r : r + step].astype(jnp.float32)
        share = parts[0, r : r + step].astype(jnp.float32)
        for p in range(1, parts.shape[0]):
            share = share + parts[p, r : r + step].astype(jnp.float32)
        x = x + share
        n = x * lax.rsqrt(jnp.mean(x * x, axis=1, keepdims=True) + EPS) * gain[...]
        for j in range(high):
            at = pl.ds(r * high + j, step, stride=high)
            state[at] = x[:, j * LANES : (j + 1) * LANES]
            normed[at] = n[:, j * LANES : (j + 1) * LANES]
    tiles[...] = normed[...].astype(jnp.bfloat16)
    places, slots = outs[0].shape[0], len(outs)

    def lay(e, _):
        for s, out in enumerate(outs):
            t = pl.multiple_of(token[e * slots + s] * high, high)
            out[e] = tiles[pl.ds(t, high)]
        return 0

    lax.fori_loop(0, places, lay, 0, unroll=8)


def settled(parts, residual, gain, token, places, slots):
    rows, width = residual.shape
    high = width // LANES
    vmem = pl.BlockSpec(memory_space=pltpu.VMEM)
    smem = pl.BlockSpec(memory_space=pltpu.SMEM)
    return pl.pallas_call(
        settle_kernel,
        out_shape=[jax.ShapeDtypeStruct((rows * high, LANES), jnp.float32)]
        + [jax.ShapeDtypeStruct((places, high, LANES), jnp.bfloat16)] * slots,
        in_specs=[vmem, vmem, vmem, smem],
        out_specs=[vmem] * (1 + slots),
        scratch_shapes=[
            pltpu.VMEM((rows * high, LANES), jnp.float32),
            pltpu.VMEM((rows * high, LANES), jnp.bfloat16),
        ],
        compiler_params=pltpu.CompilerParams(vmem_limit_bytes=6 * 1024 * 1024),
        name="settle",
    )(parts, residual, gain, token)


def expert_kernel(count, *refs):
    blocks, (w_gate, w_up, w_down) = refs[:count], refs[count : count + 3]
    outs, (x, wide) = refs[count + 3 : 2 * count + 3], refs[2 * count + 3 :]
    high = blocks[0].shape[1]
    at = 0
    for block in blocks:
        n = block.shape[0]
        wide[: n * high] = block[...].reshape(n * high, LANES).astype(jnp.float32)
        for j in range(high):
            column = wide[pl.ds(j, n, stride=high)]
            x[at : at + n, j * LANES : (j + 1) * LANES] = column.astype(jnp.bfloat16)
        at += n
    gate = jnp.dot(x[...], w_gate[...], preferred_element_type=jnp.float32)
    up = jnp.dot(x[...], w_up[...], preferred_element_type=jnp.float32)
    hidden = (gate / (1.0 + jnp.exp(-gate)) * up).astype(jnp.bfloat16)
    result = jnp.dot(hidden, w_down[...], preferred_element_type=jnp.float32)
    at = 0
    for out in outs:
        n = out.shape[0]
        for j in range(high):
            wide[pl.ds(j, n, stride=high)] = result[at : at + n, j * LANES : (j + 1) * LANES]
        out[...] = wide[: n * high].astype(jnp.bfloat16).reshape(n, high, LANES)
        at += n


def expert(blocks, w_gate, w_up, w_down):
    total = sum(b.shape[0] for b in blocks)
    most = max(b.shape[0] for b in blocks)
    high = blocks[0].shape[1]
    vmem = pl.BlockSpec(memory_space=pltpu.VMEM)
    return pl.pallas_call(
        functools.partial(expert_kernel, len(blocks)),
        out_shape=[jax.ShapeDtypeStruct(b.shape, jnp.bfloat16) for b in blocks],
        in_specs=[vmem] * (len(blocks) + 3),
        out_specs=[vmem] * len(blocks),
        scratch_shapes=[
            pltpu.VMEM((total, high * LANES), jnp.bfloat16),
            pltpu.VMEM((most * high, LANES), jnp.float32),
        ],
        compiler_params=pltpu.CompilerParams(vmem_limit_bytes=24 * 1024 * 1024),
        cost_estimate=pl.CostEstimate(
            flops=6 * total * high * LANES * w_up.shape[1],
            bytes_accessed=2 * total * high * LANES * 2,
            transcendentals=total * w_up.shape[1],
        ),
        name="expert",
    )(*blocks, w_gate, w_up, w_down)


def finish_kernel(slots, top, state, place, weight, *refs):
    returned, out, wide = refs
    rows, width = out.shape
    high = width // LANES

    def add(t, _):
        at = pl.ds(pl.multiple_of(t * high, high), high)
        y = state[at]
        for r in range(top):
            k = t * top + r
            y = y + weight[k] * returned[place[k]].astype(jnp.float32)
        wide[at] = y
        return 0

    lax.fori_loop(0, rows, add, 0, unroll=4)
    step = 16
    for r in range(0, rows, step):
        for j in range(high):
            column = wide[pl.ds(r * high + j, step, stride=high)]
            out[r : r + step, j * LANES : (j + 1) * LANES] = column.astype(jnp.bfloat16)


def finished(state, returned, place, weight, rows, top):
    high = returned.shape[1]
    vmem = pl.BlockSpec(memory_space=pltpu.VMEM)
    smem = pl.BlockSpec(memory_space=pltpu.SMEM)
    return pl.pallas_call(
        functools.partial(finish_kernel, 1, top),
        out_shape=jax.ShapeDtypeStruct((rows, high * LANES), jnp.bfloat16),
        in_specs=[vmem, smem, smem, vmem],
        out_specs=vmem,
        scratch_shapes=[pltpu.VMEM((rows * high, LANES), jnp.float32)],
        compiler_params=pltpu.CompilerParams(vmem_limit_bytes=6 * 1024 * 1024),
        name="finish",
    )(state, place, weight, returned)


def served(block, weights):
    half = block.shape[0] // 2
    behind, ahead = shifted(block, TP, 1), shifted(block, TP, -1)
    near = expert([block], *weights)
    behind, ahead, *near = lax.optimization_barrier((behind, ahead, *near))
    far = [shifted(behind[:half], TP, 1), shifted(ahead[half:], TP, -1)]
    return [*near, *expert([behind, ahead], *weights), *expert(far, *weights)]


def summed_around(parts):
    own, behind, ahead, first, second = (p.astype(jnp.float32) for p in parts)
    half = parts[3].shape[0]
    first, second = shifted(parts[3], TP, 1), shifted(parts[4], TP, -1)
    zero = jnp.zeros(first.shape, jnp.float32)
    ahead = ahead + jnp.concatenate([first.astype(jnp.float32), zero])
    behind = behind + jnp.concatenate([zero, second.astype(jnp.float32)])
    from_behind = shifted(ahead.astype(jnp.bfloat16), TP, 1)
    from_ahead = shifted(behind.astype(jnp.bfloat16), TP, -1)
    total = own + from_behind.astype(jnp.float32) + from_ahead.astype(jnp.float32)
    return total.astype(jnp.bfloat16)


def exchanged(x):
    return lax.all_to_all(x, SP, split_axis=0, concat_axis=0, tiled=True)


def local(
    queries,
    keys,
    values,
    diff_scale,
    head_gain,
    w_out,
    residual,
    norm_gain,
    route_ids,
    route_weights,
    w_gate,
    w_up,
    w_down,
):
    q_rows = queries.shape[0]
    heads_dev = diff_scale.shape[0]
    half_dim = queries.shape[1] // (2 * heads_dev)
    group_cols = keys.shape[1] // KV_HEADS
    value_cols = values.shape[1] // KV_HEADS
    swap = [(0, 1), (1, 0)]

    group, quarter = lax.axis_index("xh"), lax.axis_index("xl")
    part_rows = q_rows // 2
    k_part = lax.dynamic_slice(
        keys, (quarter * part_rows, group * group_cols), (part_rows, group_cols)
    )
    v_part = lax.dynamic_slice(
        values, (quarter * part_rows, group * value_cols), (part_rows, value_cols)
    )
    joined = jnp.concatenate([k_part, v_part], axis=1)
    q_own = jnp.stack(
        [
            jnp.concatenate(
                [
                    queries[:, (2 * h + m) * half_dim : (2 * h + m + 1) * half_dim]
                    for h in range(heads_dev)
                ]
            )
            for m in range(2)
        ]
    )

    joined, q_own = lax.optimization_barrier((joined, q_own))
    copies = jnp.broadcast_to(joined, (lax.axis_size("y"), *joined.shape))
    block = lax.all_to_all(copies, "y", split_axis=0, concat_axis=0, tiled=True)
    block = block.reshape(-1, joined.shape[1])
    q_x = lax.ppermute(q_own, "xl", swap)
    block, q_x = lax.optimization_barrier((block, q_x))
    q_pair = jnp.stack([q_own, q_x])
    q_other = lax.ppermute(q_pair, "core", swap)
    qs = [q_pair, q_other]
    scale = 1.0 / math.sqrt(half_dim)
    n = lax.axis_size("z")
    right, left = shifted(block, "z", 1), shifted(block, "z", -1)
    kvs, carry = [block, right, left], []
    for step in range(2, n // 2 + 1):
        if step == n // 2:
            right, left = shifted(right, "z", 1), None
        else:
            right, left = shifted(right, "z", 1), shifted(left, "z", -1)
        carry = attention(qs, kvs, carry, False, scale)
        kvs = [kv for kv in (right, left) if kv is not None]
        kvs, carry = lax.optimization_barrier((kvs, carry))
        right, left = kvs[0], kvs[-1]
    carry = attention(qs, kvs, carry, True, scale)
    kept, sent, kept_stat = carry
    own, own_stat, across = core_merged(kept, kept_stat, lax.ppermute(sent, "core", swap))
    came = lax.ppermute(across, "xl", swap)
    shares = projected(own, own_stat, came, diff_scale, head_gain[None, :], w_out, q_rows)
    rows_out = residual.shape[0]
    arrived = lax.all_to_all(
        cut_along(shares, 0, lax.axis_size(TP)), TP, split_axis=0, concat_axis=0, tiled=True
    )
    places = lax.axis_size(SP)
    top = route_ids.shape[1]
    slots = 2
    flat_ids = route_ids.reshape(-1)
    onehot = (flat_ids[:, None] == jnp.arange(places, dtype=jnp.int32)[None, :]).astype(jnp.int32)
    slot = jnp.sum((jnp.cumsum(onehot, axis=0) - onehot) * onehot, axis=1)
    dest = flat_ids * slots + slot
    taken = dest[:, None] == jnp.arange(places * slots, dtype=jnp.int32)[None, :]
    source = jnp.arange(flat_ids.shape[0], dtype=jnp.int32)[:, None] // top
    token = jnp.sum(jnp.where(taken, source, 0), axis=0)

    state, *outgoing = settled(arrived, residual, norm_gain[None, :], token, places, slots)
    outgoing = jnp.concatenate(outgoing, axis=1)
    high = outgoing.shape[1] // slots
    received = exchanged(outgoing).reshape(places * slots, high, LANES)
    parts = served(received, (w_gate[0], w_up[0], w_down[0]))
    back = summed_around(parts).reshape(places, slots * high, LANES)
    returned = exchanged(back).reshape(places * slots, high, LANES)
    place = dest
    return finished(state, returned, place, route_weights.reshape(-1), rows_out, top)


def solution(mesh):
    cells = mesh.devices.reshape(8, 4, 2, 2, 2)
    mesh = Mesh(cells, ("z", "y", "core", "xh", "xl"))
    in_specs = (
        P(SP, TP),
        P(SP, None),
        P(SP, None),
        P(TP),
        P(),
        P(TP, None),
        P(SP + TP, None),
        P(),
        P(SP + TP, None),
        P(SP + TP, None),
        P(SP, None, TP),
        P(SP, None, TP),
        P(SP, TP, None),
    )
    out_specs = P(SP + TP, None)
    return jax.shard_map(local, mesh=mesh, in_specs=in_specs, out_specs=out_specs, check_vma=False)
```

```python
import functools
import math

import jax
import jax.numpy as jnp
from jax import lax
from jax.experimental import pallas as pl
from jax.experimental.pallas import tpu as pltpu
from jax.sharding import Mesh
from jax.sharding import PartitionSpec as P

KV_HEADS = 2
SP = ("z", "y", "core")
TP = ("xh", "xl")


EPS = 1e-06
LOG2E = math.log2(math.e)


def cut_along(shard, dim, peers):
    before, after = (shard.shape[:dim], shard.shape[dim + 1 :])
    return jnp.moveaxis(shard.reshape(*before, peers, -1, *after), dim, 0)


def shifted(x, axis, by):
    n = lax.axis_size(axis)
    return lax.ppermute(x, axis, [(i, (i + by) % n) for i in range(n)])


STAT_ROWS = 16


def stats_block(high, total):
    line = lax.broadcasted_iota(jnp.int32, (STAT_ROWS, 256), 0)
    block = jnp.zeros((STAT_ROWS, 256), jnp.float32)
    for i, row in enumerate((high, total)):
        for k in range(3):
            part = row.astype(jnp.bfloat16).astype(jnp.float32)
            row = row - part
            tail = jnp.concatenate([part[:, 256:], part[:, 256:]], axis=1)
            block = jnp.where(line == 3 * i + k, part[:, :256], block)
            block = jnp.where(line == 6 + 3 * i + k, tail, block)
    return block.astype(jnp.bfloat16)


def stats_rows(block):
    block = block.astype(jnp.float32)
    rows = []
    for i in range(2):
        first, tail = (
            block[at : at + 1] + block[at + 1 : at + 2] + block[at + 2 : at + 3]
            for at in (3 * i, 6 + 3 * i)
        )
        rows.append(jnp.concatenate([first, tail[:, :128]], axis=1))
    return rows


def attention_kernel(n_q, n_kv, first, last, scale, *refs):
    q_refs, kv_refs = refs[:n_q], refs[n_q : n_q + n_kv]
    refs = refs[n_q + n_kv :]
    if not first:
        acc_in, high_in, total_in, *refs = refs
    if last:
        kept, sent, kept_stat, *refs = refs
    else:
        acc, high, total, *refs = refs
    q, k0, k1, v, s_a, s_b, p_a, p_b, f_a, f_b, h_a, h_b, t_a, t_b = refs
    ks = (k0, k1)
    at = 0
    for ref in kv_refs:
        n = ref.shape[0]
        k0[at : at + n] = ref[:, :128]
        k1[at : at + n] = ref[:, 128:256]
        v[at : at + n] = ref[:, 256:]
        at += n
    for i, ref in enumerate(q_refs):
        q[2 * i : 2 * i + 2] = ref[...]
    pieces, _, rows, _ = q.shape
    sub = 16
    c = scale * LOG2E
    keep = pieces // 2

    def score(i, m, s):
        s[...] = lax.dot_general(
            q[i, m], ks[m][...], (((1,), (1,)), ((), ())), preferred_element_type=jnp.float32
        )

    def soft(i, m, s, p, f, h, t, stat):
        n = s.shape[1] // 128
        if not first:
            h[0] = high_in[i, m]
            t[0] = total_in[i, m]
        for r in range(0, rows, sub):
            part = slice(r, r + sub)
            x = [s[part, g * 128 : (g + 1) * 128] for g in range(n)]
            top = jnp.max(functools.reduce(jnp.maximum, x), axis=1, keepdims=True)
            peak = jnp.broadcast_to(top, (sub, 128))
            if not first:
                before = h[0, part]
                peak = jnp.maximum(before, peak)
                fade = jnp.exp2((before - peak) * c)
                f[part] = fade
            e = [jnp.exp2((y - peak) * c) for y in x]
            for g in range(n):
                p[part, g * 128 : (g + 1) * 128] = e[g].astype(jnp.bfloat16)
            count = functools.reduce(jnp.add, e)
            if last:
                count = count + t[0, part] * fade * (1.0 / 128)
            else:
                count = jnp.broadcast_to(jnp.sum(count, axis=1, keepdims=True), (sub, 128))
                if not first:
                    count = count + t[0, part] * fade
            h[1, part] = peak * scale if last else peak
            t[1, part] = count
        if last:
            top = jnp.transpose(h[1])[0:1]
            count = jnp.sum(jnp.transpose(t[1]), axis=0, keepdims=True)
            if stat is None:
                sent[i % keep, m, rows:] = stats_block(top, count)
            else:
                line = lax.broadcasted_iota(jnp.int32, (8, rows), 0)
                stat[i * 2 + m] = jnp.where(line == 0, top, count)
        else:
            high[i, m] = h[1]
            total[i, m] = t[1]

    def mix(i, m, p, f, out):
        o = jnp.dot(p[...], v[...], preferred_element_type=jnp.float32)
        at = i % keep if last else i
        for g in range(0, o.shape[1], 128):
            part = o[:, g : g + 128]
            if not first:
                part = part + acc_in[i, m, :, g : g + 128] * f[...]
            out[at, m, :rows, g : g + 128] = part.astype(out.dtype)

    def run(start, stop, out, stat):
        score(start, 0, s_a)

        def body(i, _):
            score(i, 1, s_b)

            @pl.when(i > start)
            def _():
                mix(i - 1, 1, p_b, f_b, out)

            soft(i, 0, s_a, p_a, f_a, h_a, t_a, stat)
            score(jnp.minimum(i + 1, stop - 1), 0, s_a)
            mix(i, 0, p_a, f_a, out)
            soft(i, 1, s_b, p_b, f_b, h_b, t_b, stat)
            return 0

        lax.fori_loop(start, stop, body, 0)
        mix(stop - 1, 1, p_b, f_b, out)

    if last:
        run(keep, pieces, sent, None)
        run(0, keep, kept, kept_stat)
    else:
        run(0, pieces, acc, None)


def attention(qs, kvs, carry, last, scale):
    pieces = 2 * len(qs)
    _, _, rows, half = qs[0].shape
    n_keys = sum(kv.shape[0] for kv in kvs)
    width = kvs[0].shape[1] - 2 * half
    vmem = pl.BlockSpec(memory_space=pltpu.VMEM)
    keep = pieces // 2
    if last:
        out_shape = [
            jax.ShapeDtypeStruct((keep, 2, rows, width), jnp.float32),
            jax.ShapeDtypeStruct((keep, 2, rows + STAT_ROWS, width), jnp.bfloat16),
            jax.ShapeDtypeStruct((2 * keep, 8, rows), jnp.float32),
        ]
    else:
        out_shape = [
            jax.ShapeDtypeStruct((pieces, 2, rows, width), jnp.float32),
            jax.ShapeDtypeStruct((pieces, 2, rows, 128), jnp.float32),
            jax.ShapeDtypeStruct((pieces, 2, rows, 128), jnp.float32),
        ]
    n_in = len(qs) + len(kvs)
    aliases = {n_in + i: i for i in range(3)} if carry and not last else {}
    return pl.pallas_call(
        functools.partial(attention_kernel, len(qs), len(kvs), not carry, last, scale),
        out_shape=out_shape,
        in_specs=[vmem] * (n_in + len(carry)),
        out_specs=[vmem] * len(out_shape),
        scratch_shapes=[pltpu.VMEM((pieces, 2, rows, half), jnp.bfloat16)]
        + [pltpu.VMEM((n_keys, half), jnp.bfloat16)] * 2
        + [pltpu.VMEM((n_keys, width), jnp.bfloat16)]
        + [pltpu.VMEM((rows, n_keys), jnp.float32)] * 2
        + [pltpu.VMEM((rows, n_keys), jnp.bfloat16)] * 2
        + [pltpu.VMEM((rows, 128), jnp.float32)] * 2
        + [pltpu.VMEM((2, rows, 128), jnp.float32)] * 4,
        input_output_aliases=aliases,
        compiler_params=pltpu.CompilerParams(vmem_limit_bytes=32 * 1024 * 1024),
        cost_estimate=pl.CostEstimate(
            flops=4 * pieces * rows * n_keys * (half + width),
            bytes_accessed=n_keys * (2 * half + width) * 2,
            transcendentals=2 * pieces * rows * n_keys,
        ),
        name="attention",
    )(*qs, *kvs, *carry)


def factors(high_a, total_a, high_b, total_b):
    high = jnp.maximum(high_a, high_b)
    fade_a, fade_b = jnp.exp(high_a - high), jnp.exp(high_b - high)
    return fade_a, fade_b, high, total_a * fade_a + total_b * fade_b


def scaled_sum(a, factor_a, b, factor_b):
    rows = a.shape[0]
    fa = jnp.transpose(jnp.broadcast_to(factor_a, (128, rows)))
    fb = jnp.transpose(jnp.broadcast_to(factor_b, (128, rows)))
    parts = []
    for g in range(0, a.shape[1], 128):
        part = slice(g, g + 128)
        parts.append(a[:, part] * fa + b[:, part].astype(jnp.float32) * fb)
    return parts


def core_merge_kernel(kept, kept_stat, came, own, own_stat, across):
    rows = own.shape[1]
    line = lax.broadcasted_iota(jnp.int32, (8, rows), 0)
    for i, out in enumerate((own, across)):
        for m in range(2):
            at = 2 * i + m
            stats = stats_rows(came[i, m, rows:])
            fa, fb, high, total = factors(kept_stat[at, 0:1], kept_stat[at, 1:2], *stats)
            parts = scaled_sum(kept[i, m], fa, came[i, m, :rows], fb)
            for g, part in enumerate(parts):
                out[m, :rows, g * 128 : (g + 1) * 128] = part.astype(out.dtype)
            if i == 0:
                own_stat[m] = jnp.where(line == 0, high, total)
            else:
                across[m, rows:] = stats_block(high, total)


def core_merged(kept, kept_stat, came):
    _, _, rows, width = kept.shape
    vmem = pl.BlockSpec(memory_space=pltpu.VMEM)
    return pl.pallas_call(
        core_merge_kernel,
        out_shape=[
            jax.ShapeDtypeStruct((2, rows, width), jnp.float32),
            jax.ShapeDtypeStruct((2, 8, rows), jnp.float32),
            jax.ShapeDtypeStruct((2, rows + STAT_ROWS, width), jnp.bfloat16),
        ],
        in_specs=[vmem] * 3,
        out_specs=[vmem] * 3,
        compiler_params=pltpu.CompilerParams(vmem_limit_bytes=8 * 1024 * 1024),
        name="core_merge",
    )(kept, kept_stat, came)


def project_kernel(own, own_stat, came, diff_scale, gain, w_out, shares, head_out):
    rows, heads = shares.shape[0], diff_scale.shape[0]
    width = own.shape[2]
    maps = []
    for m in range(2):
        each = own.shape[1]
        stats = stats_rows(came[m, each:])
        fa, fb, _, total = factors(own_stat[m, 0:1], own_stat[m, 1:2], *stats)
        maps.append(scaled_sum(own[m], fa / total, came[m, :each], fb / total))
    for h in range(heads):
        part = slice(h * rows, (h + 1) * rows)
        mixed = [a[part] - diff_scale[h] * b[part] for a, b in zip(*maps)]
        mean = sum(jnp.sum(x * x, axis=1, keepdims=True) for x in mixed) / width
        norm = lax.rsqrt(mean + EPS)
        for g, x in enumerate(mixed):
            at = slice(h * width + g * 128, h * width + (g + 1) * 128)
            x = x * norm * gain[:, g * 128 : (g + 1) * 128]
            head_out[:, at] = x.astype(jnp.bfloat16)
    out = jnp.dot(head_out[...], w_out[...], preferred_element_type=jnp.float32)
    shares[...] = out.astype(jnp.bfloat16)


def projected(own, own_stat, came, diff_scale, gain, w_out, rows):
    vmem = pl.BlockSpec(memory_space=pltpu.VMEM)
    smem = pl.BlockSpec(memory_space=pltpu.SMEM)
    return pl.pallas_call(
        project_kernel,
        out_shape=jax.ShapeDtypeStruct((rows, w_out.shape[1]), jnp.bfloat16),
        in_specs=[vmem] * 3 + [smem, vmem, vmem],
        out_specs=vmem,
        scratch_shapes=[pltpu.VMEM((rows, w_out.shape[0]), jnp.bfloat16)],
        compiler_params=pltpu.CompilerParams(vmem_limit_bytes=12 * 1024 * 1024),
        name="project",
    )(own, own_stat, came, diff_scale, gain, w_out)


LANES = 128


def settle_kernel(parts, residual, gain, token, state, *refs):
    out, normed, tiles = refs
    rows, width = residual.shape
    high = width // LANES
    step = 16
    for r in range(0, rows, step):
        x = residual[r : r + step].astype(jnp.float32)
        share = parts[0, r : r + step].astype(jnp.float32)
        for p in range(1, parts.shape[0]):
            share = share + parts[p, r : r + step].astype(jnp.float32)
        x = x + share
        n = x * lax.rsqrt(jnp.mean(x * x, axis=1, keepdims=True) + EPS) * gain[...]
        for j in range(high):
            at = pl.ds(r * high + j, step, stride=high)
            state[at] = x[:, j * LANES : (j + 1) * LANES]
            normed[at] = n[:, j * LANES : (j + 1) * LANES]
    tiles[...] = normed[...].astype(jnp.bfloat16)
    places, slots = out.shape[0], out.shape[1] // high

    def lay(e, _):
        for s in range(slots):
            t = pl.multiple_of(token[e * slots + s] * high, high)
            out[e, s * high : (s + 1) * high] = tiles[pl.ds(t, high)]
        return 0

    lax.fori_loop(0, places, lay, 0, unroll=8)


def settled(parts, residual, gain, token, places, slots):
    rows, width = residual.shape
    high = width // LANES
    vmem = pl.BlockSpec(memory_space=pltpu.VMEM)
    smem = pl.BlockSpec(memory_space=pltpu.SMEM)
    return pl.pallas_call(
        settle_kernel,
        out_shape=[jax.ShapeDtypeStruct((rows * high, LANES), jnp.float32)]
        + [jax.ShapeDtypeStruct((places, slots * high, LANES), jnp.bfloat16)],
        in_specs=[vmem, vmem, vmem, smem],
        out_specs=[vmem] * 2,
        scratch_shapes=[
            pltpu.VMEM((rows * high, LANES), jnp.float32),
            pltpu.VMEM((rows * high, LANES), jnp.bfloat16),
        ],
        compiler_params=pltpu.CompilerParams(vmem_limit_bytes=6 * 1024 * 1024),
        name="settle",
    )(parts, residual, gain, token)


def expert_kernel(count, *refs):
    blocks, (w_gate, w_up, w_down) = refs[:count], refs[count : count + 3]
    outs, (x, wide) = refs[count + 3 : 2 * count + 3], refs[2 * count + 3 :]
    high = blocks[0].shape[1]
    at = 0
    for block in blocks:
        n = block.shape[0]
        wide[: n * high] = block[...].reshape(n * high, LANES).astype(jnp.float32)
        for j in range(high):
            column = wide[pl.ds(j, n, stride=high)]
            x[at : at + n, j * LANES : (j + 1) * LANES] = column.astype(jnp.bfloat16)
        at += n
    gate = jnp.dot(x[...], w_gate[...], preferred_element_type=jnp.float32)
    up = jnp.dot(x[...], w_up[...], preferred_element_type=jnp.float32)
    hidden = (gate / (1.0 + jnp.exp(-gate)) * up).astype(jnp.bfloat16)
    result = jnp.dot(hidden, w_down[...], preferred_element_type=jnp.float32)
    at = 0
    for out in outs:
        n = out.shape[0]
        for j in range(high):
            wide[pl.ds(j, n, stride=high)] = result[at : at + n, j * LANES : (j + 1) * LANES]
        out[...] = wide[: n * high].astype(jnp.bfloat16).reshape(n, high, LANES)
        at += n


def expert(blocks, w_gate, w_up, w_down):
    total = sum(b.shape[0] for b in blocks)
    most = max(b.shape[0] for b in blocks)
    high = blocks[0].shape[1]
    vmem = pl.BlockSpec(memory_space=pltpu.VMEM)
    return pl.pallas_call(
        functools.partial(expert_kernel, len(blocks)),
        out_shape=[jax.ShapeDtypeStruct(b.shape, jnp.bfloat16) for b in blocks],
        in_specs=[vmem] * (len(blocks) + 3),
        out_specs=[vmem] * len(blocks),
        scratch_shapes=[
            pltpu.VMEM((total, high * LANES), jnp.bfloat16),
            pltpu.VMEM((most * high, LANES), jnp.float32),
        ],
        compiler_params=pltpu.CompilerParams(vmem_limit_bytes=24 * 1024 * 1024),
        cost_estimate=pl.CostEstimate(
            flops=6 * total * high * LANES * w_up.shape[1],
            bytes_accessed=2 * total * high * LANES * 2,
            transcendentals=total * w_up.shape[1],
        ),
        name="expert",
    )(*blocks, w_gate, w_up, w_down)


def finish_kernel(slots, top, state, place, weight, *refs):
    returned, out, wide = refs
    rows, width = out.shape
    high = width // LANES

    def add(t, _):
        at = pl.ds(pl.multiple_of(t * high, high), high)
        y = state[at]
        for r in range(top):
            k = t * top + r
            y = y + weight[k] * returned[place[k]].astype(jnp.float32)
        wide[at] = y
        return 0

    lax.fori_loop(0, rows, add, 0, unroll=4)
    step = 16
    for r in range(0, rows, step):
        for j in range(high):
            column = wide[pl.ds(r * high + j, step, stride=high)]
            out[r : r + step, j * LANES : (j + 1) * LANES] = column.astype(jnp.bfloat16)


def finished(state, returned, place, weight, rows, top):
    high = returned.shape[1]
    vmem = pl.BlockSpec(memory_space=pltpu.VMEM)
    smem = pl.BlockSpec(memory_space=pltpu.SMEM)
    return pl.pallas_call(
        functools.partial(finish_kernel, 1, top),
        out_shape=jax.ShapeDtypeStruct((rows, high * LANES), jnp.bfloat16),
        in_specs=[vmem, smem, smem, vmem],
        out_specs=vmem,
        scratch_shapes=[pltpu.VMEM((rows * high, LANES), jnp.float32)],
        compiler_params=pltpu.CompilerParams(vmem_limit_bytes=6 * 1024 * 1024),
        name="finish",
    )(state, place, weight, returned)


def served(block, weights):
    half = block.shape[0] // 2
    behind, ahead = shifted(block, TP, 1), shifted(block, TP, -1)
    near = expert([block], *weights)
    behind, ahead, *near = lax.optimization_barrier((behind, ahead, *near))
    far = [shifted(behind[:half], TP, 1), shifted(ahead[half:], TP, -1)]
    return [*near, *expert([behind, ahead], *weights), *expert(far, *weights)]


def summed_around(parts):
    own, behind, ahead, first, second = (p.astype(jnp.float32) for p in parts)
    half = parts[3].shape[0]
    first, second = shifted(parts[3], TP, 1), shifted(parts[4], TP, -1)
    zero = jnp.zeros(first.shape, jnp.float32)
    ahead = ahead + jnp.concatenate([first.astype(jnp.float32), zero])
    behind = behind + jnp.concatenate([zero, second.astype(jnp.float32)])
    from_behind = shifted(ahead.astype(jnp.bfloat16), TP, 1)
    from_ahead = shifted(behind.astype(jnp.bfloat16), TP, -1)
    total = own + from_behind.astype(jnp.float32) + from_ahead.astype(jnp.float32)
    return total.astype(jnp.bfloat16)


def exchanged(x):
    return lax.all_to_all(x, SP, split_axis=0, concat_axis=0, tiled=True)


def local(
    queries,
    keys,
    values,
    diff_scale,
    head_gain,
    w_out,
    residual,
    norm_gain,
    route_ids,
    route_weights,
    w_gate,
    w_up,
    w_down,
):
    q_rows = queries.shape[0]
    heads_dev = diff_scale.shape[0]
    half_dim = queries.shape[1] // (2 * heads_dev)
    group_cols = keys.shape[1] // KV_HEADS
    value_cols = values.shape[1] // KV_HEADS
    swap = [(0, 1), (1, 0)]

    group, quarter = lax.axis_index("xh"), lax.axis_index("xl")
    part_rows = q_rows // 2

    def own_part(x, cols):
        x = jnp.where(group == 0, x[:, :cols], x[:, cols:])
        return jnp.where(quarter == 0, x[:part_rows], x[part_rows:])

    k_part, v_part = own_part(keys, group_cols), own_part(values, value_cols)
    joined = jnp.concatenate([k_part, v_part], axis=1)
    q_own = jnp.stack(
        [
            jnp.concatenate(
                [
                    queries[:, (2 * h + m) * half_dim : (2 * h + m + 1) * half_dim]
                    for h in range(heads_dev)
                ]
            )
            for m in range(2)
        ]
    )

    joined, q_own = lax.optimization_barrier((joined, q_own))
    copies = jnp.broadcast_to(joined, (lax.axis_size("y"), *joined.shape))
    block = lax.all_to_all(copies, "y", split_axis=0, concat_axis=0, tiled=True)
    block = block.reshape(-1, joined.shape[1])
    q_x = lax.ppermute(q_own, "xl", swap)
    block, q_x = lax.optimization_barrier((block, q_x))
    q_pair = jnp.stack([q_own, q_x])
    q_other = lax.ppermute(q_pair, "core", swap)
    qs = [q_pair, q_other]
    scale = 1.0 / math.sqrt(half_dim)
    n = lax.axis_size("z")
    right, left = shifted(block, "z", 1), shifted(block, "z", -1)
    kvs, carry = [block, right, left], []
    for step in range(2, n // 2 + 1):
        if step == n // 2:
            right, left = shifted(right, "z", 1), None
        else:
            right, left = shifted(right, "z", 1), shifted(left, "z", -1)
        carry = attention(qs, kvs, carry, False, scale)
        kvs = [kv for kv in (right, left) if kv is not None]
        kvs, carry = lax.optimization_barrier((kvs, carry))
        right, left = kvs[0], kvs[-1]
    carry = attention(qs, kvs, carry, True, scale)
    kept, sent, kept_stat = carry
    own, own_stat, across = core_merged(kept, kept_stat, lax.ppermute(sent, "core", swap))
    came = lax.ppermute(across, "xl", swap)
    shares = projected(own, own_stat, came, diff_scale, head_gain[None, :], w_out, q_rows)
    rows_out = residual.shape[0]
    arrived = lax.all_to_all(
        cut_along(shares, 0, lax.axis_size(TP)), TP, split_axis=0, concat_axis=0, tiled=True
    )
    places = lax.axis_size(SP)
    top = route_ids.shape[1]
    slots = 2
    flat_ids = route_ids.reshape(-1)
    onehot = (flat_ids[:, None] == jnp.arange(places, dtype=jnp.int32)[None, :]).astype(jnp.int32)
    slot = jnp.sum((jnp.cumsum(onehot, axis=0) - onehot) * onehot, axis=1)
    dest = flat_ids * slots + slot
    taken = dest[:, None] == jnp.arange(places * slots, dtype=jnp.int32)[None, :]
    source = jnp.arange(flat_ids.shape[0], dtype=jnp.int32)[:, None] // top
    token = jnp.sum(jnp.where(taken, source, 0), axis=0)

    state, outgoing = settled(arrived, residual, norm_gain[None, :], token, places, slots)
    high = outgoing.shape[1] // slots
    received = exchanged(outgoing).reshape(places * slots, high, LANES)
    parts = served(received, (w_gate[0], w_up[0], w_down[0]))
    back = summed_around(parts).reshape(places, slots * high, LANES)
    returned = exchanged(back).reshape(places * slots, high, LANES)
    place = dest
    return finished(state, returned, place, route_weights.reshape(-1), rows_out, top)


def solution(mesh):
    cells = mesh.devices.reshape(8, 4, 2, 2, 2)
    mesh = Mesh(cells, ("z", "y", "core", "xh", "xl"))
    in_specs = (
        P(SP, TP),
        P(SP, None),
        P(SP, None),
        P(TP),
        P(),
        P(TP, None),
        P(SP + TP, None),
        P(),
        P(SP + TP, None),
        P(SP + TP, None),
        P(SP, None, TP),
        P(SP, None, TP),
        P(SP, TP, None),
    )
    out_specs = P(SP + TP, None)
    return jax.shard_map(local, mesh=mesh, in_specs=in_specs, out_specs=out_specs, check_vma=False)
```

```python
import functools
import math

import jax
import jax.numpy as jnp
from jax import lax
from jax.experimental import pallas as pl
from jax.experimental.pallas import tpu as pltpu
from jax.sharding import Mesh
from jax.sharding import PartitionSpec as P

KV_HEADS = 2
SP = ("z", "y", "core")
TP = ("xh", "xl")


EPS = 1e-06
LOG2E = math.log2(math.e)


def cut_along(shard, dim, peers):
    before, after = (shard.shape[:dim], shard.shape[dim + 1 :])
    return jnp.moveaxis(shard.reshape(*before, peers, -1, *after), dim, 0)


def shifted(x, axis, by):
    n = lax.axis_size(axis)
    return lax.ppermute(x, axis, [(i, (i + by) % n) for i in range(n)])


STAT_ROWS = 16


def stats_block(high, total):
    line = lax.broadcasted_iota(jnp.int32, (STAT_ROWS, 256), 0)
    block = jnp.zeros((STAT_ROWS, 256), jnp.float32)
    for i, row in enumerate((high, total)):
        for k in range(3):
            part = row.astype(jnp.bfloat16).astype(jnp.float32)
            row = row - part
            tail = jnp.concatenate([part[:, 256:], part[:, 256:]], axis=1)
            block = jnp.where(line == 3 * i + k, part[:, :256], block)
            block = jnp.where(line == 6 + 3 * i + k, tail, block)
    return block.astype(jnp.bfloat16)


def stats_rows(block):
    block = block.astype(jnp.float32)
    rows = []
    for i in range(2):
        first, tail = (
            block[at : at + 1] + block[at + 1 : at + 2] + block[at + 2 : at + 3]
            for at in (3 * i, 6 + 3 * i)
        )
        rows.append(jnp.concatenate([first, tail[:, :128]], axis=1))
    return rows


def attention_kernel(n_q, n_kv, first, last, base, scale, *refs):
    q_refs, kv_refs = refs[:n_q], refs[n_q : n_q + n_kv]
    refs = refs[n_q + n_kv :]
    if not first:
        acc_in, high_in, total_in, *refs = refs
    kept_stat = None
    if last == "sent":
        sent, *refs = refs
    elif last == "kept":
        kept, kept_stat, *refs = refs
    else:
        acc, high, total, *refs = refs
    q, k0, k1, v, s_a, s_b, p_a, p_b, f_a, f_b, h_a, h_b, t_a, t_b = refs
    ks = (k0, k1)
    at = 0
    for ref in kv_refs:
        n = ref.shape[0]
        k0[at : at + n] = ref[:, :128]
        k1[at : at + n] = ref[:, 128:256]
        v[at : at + n] = ref[:, 256:]
        at += n
    for i, ref in enumerate(q_refs):
        q[2 * i : 2 * i + 2] = ref[...]
    pieces, _, rows, _ = q.shape
    sub = 16
    c = scale * LOG2E

    def score(i, m, s):
        s[...] = lax.dot_general(
            q[i, m], ks[m][...], (((1,), (1,)), ((), ())), preferred_element_type=jnp.float32
        )

    def soft(i, m, s, p, f, h, t, stat):
        n = s.shape[1] // 128
        if not first:
            h[0] = high_in[i + base, m]
            t[0] = total_in[i + base, m]
        for r in range(0, rows, sub):
            part = slice(r, r + sub)
            x = [s[part, g * 128 : (g + 1) * 128] for g in range(n)]
            top = jnp.max(functools.reduce(jnp.maximum, x), axis=1, keepdims=True)
            peak = jnp.broadcast_to(top, (sub, 128))
            if not first:
                before = h[0, part]
                peak = jnp.maximum(before, peak)
                fade = jnp.exp2((before - peak) * c)
                f[part] = fade
            e = [jnp.exp2((y - peak) * c) for y in x]
            for g in range(n):
                p[part, g * 128 : (g + 1) * 128] = e[g].astype(jnp.bfloat16)
            count = functools.reduce(jnp.add, e)
            if last:
                count = count + t[0, part] * fade * (1.0 / 128)
            else:
                count = jnp.broadcast_to(jnp.sum(count, axis=1, keepdims=True), (sub, 128))
                if not first:
                    count = count + t[0, part] * fade
            h[1, part] = peak * scale if last else peak
            t[1, part] = count
        if last:
            top = jnp.transpose(h[1])[0:1]
            count = jnp.sum(jnp.transpose(t[1]), axis=0, keepdims=True)
            if stat is None:
                sent[i, m, rows:] = stats_block(top, count)
            else:
                line = lax.broadcasted_iota(jnp.int32, (8, rows), 0)
                stat[i * 2 + m] = jnp.where(line == 0, top, count)
        else:
            high[i, m] = h[1]
            total[i, m] = t[1]

    def mix(i, m, p, f, out):
        o = jnp.dot(p[...], v[...], preferred_element_type=jnp.float32)
        for g in range(0, o.shape[1], 128):
            part = o[:, g : g + 128]
            if not first:
                part = part + acc_in[i + base, m, :, g : g + 128] * f[...]
            out[i, m, :rows, g : g + 128] = part.astype(out.dtype)

    def run(start, stop, out, stat):
        score(start, 0, s_a)

        def body(i, _):
            score(i, 1, s_b)

            @pl.when(i > start)
            def _():
                mix(i - 1, 1, p_b, f_b, out)

            soft(i, 0, s_a, p_a, f_a, h_a, t_a, stat)
            score(jnp.minimum(i + 1, stop - 1), 0, s_a)
            mix(i, 0, p_a, f_a, out)
            soft(i, 1, s_b, p_b, f_b, h_b, t_b, stat)
            return 0

        lax.fori_loop(start, stop, body, 0)
        mix(stop - 1, 1, p_b, f_b, out)

    if last == "sent":
        run(0, pieces, sent, None)
    elif last == "kept":
        run(0, pieces, kept, kept_stat)
    else:
        run(0, pieces, acc, None)


def attention(qs, kvs, carry, last, base, scale):
    pieces = 2 * len(qs)
    _, _, rows, half = qs[0].shape
    n_keys = sum(kv.shape[0] for kv in kvs)
    width = kvs[0].shape[1] - 2 * half
    vmem = pl.BlockSpec(memory_space=pltpu.VMEM)
    if last == "sent":
        out_shape = [
            jax.ShapeDtypeStruct((pieces, 2, rows + STAT_ROWS, width), jnp.bfloat16),
        ]
    elif last == "kept":
        out_shape = [
            jax.ShapeDtypeStruct((pieces, 2, rows, width), jnp.float32),
            jax.ShapeDtypeStruct((2 * pieces, 8, rows), jnp.float32),
        ]
    else:
        out_shape = [
            jax.ShapeDtypeStruct((pieces, 2, rows, width), jnp.float32),
            jax.ShapeDtypeStruct((pieces, 2, rows, 128), jnp.float32),
            jax.ShapeDtypeStruct((pieces, 2, rows, 128), jnp.float32),
        ]
    n_in = len(qs) + len(kvs)
    aliases = {n_in + i: i for i in range(3)} if carry and not last else {}
    return pl.pallas_call(
        functools.partial(attention_kernel, len(qs), len(kvs), not carry, last, base, scale),
        out_shape=out_shape,
        in_specs=[vmem] * (n_in + len(carry)),
        out_specs=[vmem] * len(out_shape),
        scratch_shapes=[pltpu.VMEM((pieces, 2, rows, half), jnp.bfloat16)]
        + [pltpu.VMEM((n_keys, half), jnp.bfloat16)] * 2
        + [pltpu.VMEM((n_keys, width), jnp.bfloat16)]
        + [pltpu.VMEM((rows, n_keys), jnp.float32)] * 2
        + [pltpu.VMEM((rows, n_keys), jnp.bfloat16)] * 2
        + [pltpu.VMEM((rows, 128), jnp.float32)] * 2
        + [pltpu.VMEM((2, rows, 128), jnp.float32)] * 4,
        input_output_aliases=aliases,
        compiler_params=pltpu.CompilerParams(vmem_limit_bytes=32 * 1024 * 1024),
        cost_estimate=pl.CostEstimate(
            flops=4 * pieces * rows * n_keys * (half + width),
            bytes_accessed=n_keys * (2 * half + width) * 2,
            transcendentals=2 * pieces * rows * n_keys,
        ),
        name="attention",
    )(*qs, *kvs, *carry)


def factors(high_a, total_a, high_b, total_b):
    high = jnp.maximum(high_a, high_b)
    fade_a, fade_b = jnp.exp(high_a - high), jnp.exp(high_b - high)
    return fade_a, fade_b, high, total_a * fade_a + total_b * fade_b


def scaled_sum(a, factor_a, b, factor_b):
    rows = a.shape[0]
    fa = jnp.transpose(jnp.broadcast_to(factor_a, (128, rows)))
    fb = jnp.transpose(jnp.broadcast_to(factor_b, (128, rows)))
    parts = []
    for g in range(0, a.shape[1], 128):
        part = slice(g, g + 128)
        parts.append(a[:, part] * fa + b[:, part].astype(jnp.float32) * fb)
    return parts


def core_merge_kernel(kept, kept_stat, came, own, own_stat, across):
    rows = own.shape[1]
    line = lax.broadcasted_iota(jnp.int32, (8, rows), 0)
    for i, out in enumerate((own, across)):
        for m in range(2):
            at = 2 * i + m
            stats = stats_rows(came[i, m, rows:])
            fa, fb, high, total = factors(kept_stat[at, 0:1], kept_stat[at, 1:2], *stats)
            parts = scaled_sum(kept[i, m], fa, came[i, m, :rows], fb)
            for g, part in enumerate(parts):
                out[m, :rows, g * 128 : (g + 1) * 128] = part.astype(out.dtype)
            if i == 0:
                own_stat[m] = jnp.where(line == 0, high, total)
            else:
                across[m, rows:] = stats_block(high, total)


def core_merged(kept, kept_stat, came):
    _, _, rows, width = kept.shape
    vmem = pl.BlockSpec(memory_space=pltpu.VMEM)
    return pl.pallas_call(
        core_merge_kernel,
        out_shape=[
            jax.ShapeDtypeStruct((2, rows, width), jnp.float32),
            jax.ShapeDtypeStruct((2, 8, rows), jnp.float32),
            jax.ShapeDtypeStruct((2, rows + STAT_ROWS, width), jnp.bfloat16),
        ],
        in_specs=[vmem] * 3,
        out_specs=[vmem] * 3,
        compiler_params=pltpu.CompilerParams(vmem_limit_bytes=8 * 1024 * 1024),
        name="core_merge",
    )(kept, kept_stat, came)


def project_kernel(own, own_stat, came, diff_scale, gain, w_out, shares, head_out):
    rows, heads = shares.shape[0], diff_scale.shape[0]
    width = own.shape[2]
    maps = []
    for m in range(2):
        each = own.shape[1]
        stats = stats_rows(came[m, each:])
        fa, fb, _, total = factors(own_stat[m, 0:1], own_stat[m, 1:2], *stats)
        maps.append(scaled_sum(own[m], fa / total, came[m, :each], fb / total))
    for h in range(heads):
        part = slice(h * rows, (h + 1) * rows)
        mixed = [a[part] - diff_scale[h] * b[part] for a, b in zip(*maps)]
        mean = sum(jnp.sum(x * x, axis=1, keepdims=True) for x in mixed) / width
        norm = lax.rsqrt(mean + EPS)
        for g, x in enumerate(mixed):
            at = slice(h * width + g * 128, h * width + (g + 1) * 128)
            x = x * norm * gain[:, g * 128 : (g + 1) * 128]
            head_out[:, at] = x.astype(jnp.bfloat16)
    out = jnp.dot(head_out[...], w_out[...], preferred_element_type=jnp.float32)
    shares[...] = out.astype(jnp.bfloat16)


def projected(own, own_stat, came, diff_scale, gain, w_out, rows):
    vmem = pl.BlockSpec(memory_space=pltpu.VMEM)
    smem = pl.BlockSpec(memory_space=pltpu.SMEM)
    return pl.pallas_call(
        project_kernel,
        out_shape=jax.ShapeDtypeStruct((rows, w_out.shape[1]), jnp.bfloat16),
        in_specs=[vmem] * 3 + [smem, vmem, vmem],
        out_specs=vmem,
        scratch_shapes=[pltpu.VMEM((rows, w_out.shape[0]), jnp.bfloat16)],
        compiler_params=pltpu.CompilerParams(vmem_limit_bytes=12 * 1024 * 1024),
        name="project",
    )(own, own_stat, came, diff_scale, gain, w_out)


LANES = 128


def settle_kernel(parts, residual, gain, token, state, *refs):
    out, normed, tiles = refs
    rows, width = residual.shape
    high = width // LANES
    step = 16
    for r in range(0, rows, step):
        x = residual[r : r + step].astype(jnp.float32)
        share = parts[0, r : r + step].astype(jnp.float32)
        for p in range(1, parts.shape[0]):
            share = share + parts[p, r : r + step].astype(jnp.float32)
        x = x + share
        n = x * lax.rsqrt(jnp.mean(x * x, axis=1, keepdims=True) + EPS) * gain[...]
        for j in range(high):
            at = pl.ds(r * high + j, step, stride=high)
            state[at] = x[:, j * LANES : (j + 1) * LANES]
            normed[at] = n[:, j * LANES : (j + 1) * LANES]
    tiles[...] = normed[...].astype(jnp.bfloat16)
    places, slots = out.shape[0], out.shape[1] // high

    def lay(e, _):
        for s in range(slots):
            t = pl.multiple_of(token[e * slots + s] * high, high)
            out[e, s * high : (s + 1) * high] = tiles[pl.ds(t, high)]
        return 0

    lax.fori_loop(0, places, lay, 0, unroll=8)


def settled(parts, residual, gain, token, places, slots):
    rows, width = residual.shape
    high = width // LANES
    vmem = pl.BlockSpec(memory_space=pltpu.VMEM)
    smem = pl.BlockSpec(memory_space=pltpu.SMEM)
    return pl.pallas_call(
        settle_kernel,
        out_shape=[jax.ShapeDtypeStruct((rows * high, LANES), jnp.float32)]
        + [jax.ShapeDtypeStruct((places, slots * high, LANES), jnp.bfloat16)],
        in_specs=[vmem, vmem, vmem, smem],
        out_specs=[vmem] * 2,
        scratch_shapes=[
            pltpu.VMEM((rows * high, LANES), jnp.float32),
            pltpu.VMEM((rows * high, LANES), jnp.bfloat16),
        ],
        compiler_params=pltpu.CompilerParams(vmem_limit_bytes=6 * 1024 * 1024),
        name="settle",
    )(parts, residual, gain, token)


def expert_kernel(count, *refs):
    blocks, (w_gate, w_up, w_down) = refs[:count], refs[count : count + 3]
    outs, (x, wide) = refs[count + 3 : 2 * count + 3], refs[2 * count + 3 :]
    high = blocks[0].shape[1]
    at = 0
    for block in blocks:
        n = block.shape[0]
        wide[: n * high] = block[...].reshape(n * high, LANES).astype(jnp.float32)
        for j in range(high):
            column = wide[pl.ds(j, n, stride=high)]
            x[at : at + n, j * LANES : (j + 1) * LANES] = column.astype(jnp.bfloat16)
        at += n
    gate = jnp.dot(x[...], w_gate[...], preferred_element_type=jnp.float32)
    up = jnp.dot(x[...], w_up[...], preferred_element_type=jnp.float32)
    hidden = (gate / (1.0 + jnp.exp(-gate)) * up).astype(jnp.bfloat16)
    result = jnp.dot(hidden, w_down[...], preferred_element_type=jnp.float32)
    at = 0
    for out in outs:
        n = out.shape[0]
        for j in range(high):
            wide[pl.ds(j, n, stride=high)] = result[at : at + n, j * LANES : (j + 1) * LANES]
        out[...] = wide[: n * high].astype(jnp.bfloat16).reshape(n, high, LANES)
        at += n


def expert(blocks, w_gate, w_up, w_down):
    total = sum(b.shape[0] for b in blocks)
    most = max(b.shape[0] for b in blocks)
    high = blocks[0].shape[1]
    vmem = pl.BlockSpec(memory_space=pltpu.VMEM)
    return pl.pallas_call(
        functools.partial(expert_kernel, len(blocks)),
        out_shape=[jax.ShapeDtypeStruct(b.shape, jnp.bfloat16) for b in blocks],
        in_specs=[vmem] * (len(blocks) + 3),
        out_specs=[vmem] * len(blocks),
        scratch_shapes=[
            pltpu.VMEM((total, high * LANES), jnp.bfloat16),
            pltpu.VMEM((most * high, LANES), jnp.float32),
        ],
        compiler_params=pltpu.CompilerParams(vmem_limit_bytes=24 * 1024 * 1024),
        cost_estimate=pl.CostEstimate(
            flops=6 * total * high * LANES * w_up.shape[1],
            bytes_accessed=2 * total * high * LANES * 2,
            transcendentals=total * w_up.shape[1],
        ),
        name="expert",
    )(*blocks, w_gate, w_up, w_down)


def finish_kernel(slots, top, state, place, weight, *refs):
    returned, out, wide = refs
    rows, width = out.shape
    high = width // LANES

    def add(t, _):
        at = pl.ds(pl.multiple_of(t * high, high), high)
        y = state[at]
        for r in range(top):
            k = t * top + r
            y = y + weight[k] * returned[place[k]].astype(jnp.float32)
        wide[at] = y
        return 0

    lax.fori_loop(0, rows, add, 0, unroll=4)
    step = 16
    for r in range(0, rows, step):
        for j in range(high):
            column = wide[pl.ds(r * high + j, step, stride=high)]
            out[r : r + step, j * LANES : (j + 1) * LANES] = column.astype(jnp.bfloat16)


def finished(state, returned, place, weight, rows, top):
    high = returned.shape[1]
    vmem = pl.BlockSpec(memory_space=pltpu.VMEM)
    smem = pl.BlockSpec(memory_space=pltpu.SMEM)
    return pl.pallas_call(
        functools.partial(finish_kernel, 1, top),
        out_shape=jax.ShapeDtypeStruct((rows, high * LANES), jnp.bfloat16),
        in_specs=[vmem, smem, smem, vmem],
        out_specs=vmem,
        scratch_shapes=[pltpu.VMEM((rows * high, LANES), jnp.float32)],
        compiler_params=pltpu.CompilerParams(vmem_limit_bytes=6 * 1024 * 1024),
        name="finish",
    )(state, place, weight, returned)


def served(block, weights):
    half = block.shape[0] // 2
    behind, ahead = shifted(block, TP, 1), shifted(block, TP, -1)
    near = expert([block], *weights)
    behind, ahead, *near = lax.optimization_barrier((behind, ahead, *near))
    far = [shifted(behind[:half], TP, 1), shifted(ahead[half:], TP, -1)]
    return [*near, *expert([behind, ahead], *weights), *expert(far, *weights)]


def summed_around(parts):
    own, behind, ahead, first, second = (p.astype(jnp.float32) for p in parts)
    half = parts[3].shape[0]
    first, second = shifted(parts[3], TP, 1), shifted(parts[4], TP, -1)
    zero = jnp.zeros(first.shape, jnp.float32)
    ahead = ahead + jnp.concatenate([first.astype(jnp.float32), zero])
    behind = behind + jnp.concatenate([zero, second.astype(jnp.float32)])
    from_behind = shifted(ahead.astype(jnp.bfloat16), TP, 1)
    from_ahead = shifted(behind.astype(jnp.bfloat16), TP, -1)
    total = own + from_behind.astype(jnp.float32) + from_ahead.astype(jnp.float32)
    return total.astype(jnp.bfloat16)


def exchanged(x):
    return lax.all_to_all(x, SP, split_axis=0, concat_axis=0, tiled=True)


def local(
    queries,
    keys,
    values,
    diff_scale,
    head_gain,
    w_out,
    residual,
    norm_gain,
    route_ids,
    route_weights,
    w_gate,
    w_up,
    w_down,
):
    q_rows = queries.shape[0]
    heads_dev = diff_scale.shape[0]
    half_dim = queries.shape[1] // (2 * heads_dev)
    group_cols = keys.shape[1] // KV_HEADS
    value_cols = values.shape[1] // KV_HEADS
    swap = [(0, 1), (1, 0)]

    group, quarter = lax.axis_index("xh"), lax.axis_index("xl")
    part_rows = q_rows // 2

    def own_part(x, cols):
        x = jnp.where(group == 0, x[:, :cols], x[:, cols:])
        return jnp.where(quarter == 0, x[:part_rows], x[part_rows:])

    k_part, v_part = own_part(keys, group_cols), own_part(values, value_cols)
    joined = jnp.concatenate([k_part, v_part], axis=1)
    q_own = jnp.stack(
        [
            jnp.concatenate(
                [
                    queries[:, (2 * h + m) * half_dim : (2 * h + m + 1) * half_dim]
                    for h in range(heads_dev)
                ]
            )
            for m in range(2)
        ]
    )

    joined, q_own = lax.optimization_barrier((joined, q_own))
    copies = jnp.broadcast_to(joined, (lax.axis_size("y"), *joined.shape))
    block = lax.all_to_all(copies, "y", split_axis=0, concat_axis=0, tiled=True)
    block = block.reshape(-1, joined.shape[1])
    q_x = lax.ppermute(q_own, "xl", swap)
    block, q_x = lax.optimization_barrier((block, q_x))
    q_pair = jnp.stack([q_own, q_x])
    q_other = lax.ppermute(q_pair, "core", swap)
    qs = [q_pair, q_other]
    scale = 1.0 / math.sqrt(half_dim)
    n = lax.axis_size("z")
    right, left = shifted(block, "z", 1), shifted(block, "z", -1)
    kvs, carry = [block, right, left], []
    for step in range(2, n // 2 + 1):
        if step == n // 2:
            right, left = shifted(right, "z", 1), None
        else:
            right, left = shifted(right, "z", 1), shifted(left, "z", -1)
        carry = attention(qs, kvs, carry, "", 0, scale)
        kvs = [kv for kv in (right, left) if kv is not None]
        kvs, carry = lax.optimization_barrier((kvs, carry))
        right, left = kvs[0], kvs[-1]
    (sent,) = attention(qs[1:], kvs, carry, "sent", 2, scale)
    sent, *carry = lax.optimization_barrier((sent, *carry))
    sent = lax.ppermute(sent, "core", swap)
    kept, kept_stat = attention(qs[:1], kvs, carry, "kept", 0, scale)
    own, own_stat, across = core_merged(kept, kept_stat, sent)
    came = lax.ppermute(across, "xl", swap)
    shares = projected(own, own_stat, came, diff_scale, head_gain[None, :], w_out, q_rows)
    rows_out = residual.shape[0]
    arrived = lax.all_to_all(
        cut_along(shares, 0, lax.axis_size(TP)), TP, split_axis=0, concat_axis=0, tiled=True
    )
    places = lax.axis_size(SP)
    top = route_ids.shape[1]
    slots = 2
    flat_ids = route_ids.reshape(-1)
    onehot = (flat_ids[:, None] == jnp.arange(places, dtype=jnp.int32)[None, :]).astype(jnp.int32)
    slot = jnp.sum((jnp.cumsum(onehot, axis=0) - onehot) * onehot, axis=1)
    dest = flat_ids * slots + slot
    taken = dest[:, None] == jnp.arange(places * slots, dtype=jnp.int32)[None, :]
    source = jnp.arange(flat_ids.shape[0], dtype=jnp.int32)[:, None] // top
    token = jnp.sum(jnp.where(taken, source, 0), axis=0)

    state, outgoing = settled(arrived, residual, norm_gain[None, :], token, places, slots)
    high = outgoing.shape[1] // slots
    received = exchanged(outgoing).reshape(places * slots, high, LANES)
    parts = served(received, (w_gate[0], w_up[0], w_down[0]))
    back = summed_around(parts).reshape(places, slots * high, LANES)
    returned = exchanged(back).reshape(places * slots, high, LANES)
    place = dest
    return finished(state, returned, place, route_weights.reshape(-1), rows_out, top)


def solution(mesh):
    cells = mesh.devices.reshape(8, 4, 2, 2, 2)
    mesh = Mesh(cells, ("z", "y", "core", "xh", "xl"))
    in_specs = (
        P(SP, TP),
        P(SP, None),
        P(SP, None),
        P(TP),
        P(),
        P(TP, None),
        P(SP + TP, None),
        P(),
        P(SP + TP, None),
        P(SP + TP, None),
        P(SP, None, TP),
        P(SP, None, TP),
        P(SP, TP, None),
    )
    out_specs = P(SP + TP, None)
    return jax.shard_map(local, mesh=mesh, in_specs=in_specs, out_specs=out_specs, check_vma=False)
```

```python
import functools
import math

import jax
import jax.numpy as jnp
from jax import lax
from jax.experimental import pallas as pl
from jax.experimental.pallas import tpu as pltpu
from jax.sharding import Mesh
from jax.sharding import PartitionSpec as P

KV_HEADS = 2
SP = ("z", "y", "core")
TP = ("xh", "xl")


EPS = 1e-06
LOG2E = math.log2(math.e)


def cut_along(shard, dim, peers):
    before, after = (shard.shape[:dim], shard.shape[dim + 1 :])
    return jnp.moveaxis(shard.reshape(*before, peers, -1, *after), dim, 0)


def shifted(x, axis, by):
    n = lax.axis_size(axis)
    return lax.ppermute(x, axis, [(i, (i + by) % n) for i in range(n)])


STAT_ROWS = 16


def stats_block(high, total):
    line = lax.broadcasted_iota(jnp.int32, (STAT_ROWS, 256), 0)
    block = jnp.zeros((STAT_ROWS, 256), jnp.float32)
    for i, row in enumerate((high, total)):
        for k in range(3):
            part = row.astype(jnp.bfloat16).astype(jnp.float32)
            row = row - part
            tail = jnp.concatenate([part[:, 256:], part[:, 256:]], axis=1)
            block = jnp.where(line == 3 * i + k, part[:, :256], block)
            block = jnp.where(line == 6 + 3 * i + k, tail, block)
    return block.astype(jnp.bfloat16)


def stats_rows(block):
    block = block.astype(jnp.float32)
    rows = []
    for i in range(2):
        first, tail = (
            block[at : at + 1] + block[at + 1 : at + 2] + block[at + 2 : at + 3]
            for at in (3 * i, 6 + 3 * i)
        )
        rows.append(jnp.concatenate([first, tail[:, :128]], axis=1))
    return rows


def attention_kernel(n_q, n_kv, first, last, base, scale, *refs):
    q_refs, kv_refs = refs[:n_q], refs[n_q : n_q + n_kv]
    refs = refs[n_q + n_kv :]
    if not first:
        acc_in, high_in, total_in, *refs = refs
    kept_stat = None
    if last == "sent":
        sent, *refs = refs
    elif last == "kept":
        kept, kept_stat, *refs = refs
    else:
        acc, high, total, *refs = refs
    q, k0, k1, v, s_a, s_b, p_a, p_b, f_a, f_b, h_a, h_b, t_a, t_b = refs
    ks = (k0, k1)
    at = 0
    for ref in kv_refs:
        n = ref.shape[0]
        k0[at : at + n] = ref[:, :128]
        k1[at : at + n] = ref[:, 128:256]
        v[at : at + n] = ref[:, 256:]
        at += n
    for i, ref in enumerate(q_refs):
        q[2 * i : 2 * i + 2] = ref[...]
    pieces, _, rows, _ = q.shape
    sub = 16
    c = scale * LOG2E

    def score(i, m, s):
        s[...] = lax.dot_general(
            q[i, m], ks[m][...], (((1,), (1,)), ((), ())), preferred_element_type=jnp.float32
        )

    def soft(i, m, s, p, f, h, t, stat):
        n = s.shape[1] // 128
        if not first:
            h[0] = high_in[i + base, m]
            t[0] = total_in[i + base, m]
        for r in range(0, rows, sub):
            part = slice(r, r + sub)
            x = [s[part, g * 128 : (g + 1) * 128] for g in range(n)]
            top = jnp.max(functools.reduce(jnp.maximum, x), axis=1, keepdims=True)
            peak = jnp.broadcast_to(top, (sub, 128))
            if not first:
                before = h[0, part]
                peak = jnp.maximum(before, peak)
                fade = jnp.exp2((before - peak) * c)
                f[part] = fade
            e = [jnp.exp2((y - peak) * c) for y in x]
            for g in range(n):
                p[part, g * 128 : (g + 1) * 128] = e[g].astype(jnp.bfloat16)
            count = functools.reduce(jnp.add, e)
            if last:
                count = count + t[0, part] * fade * (1.0 / 128)
            else:
                count = jnp.broadcast_to(jnp.sum(count, axis=1, keepdims=True), (sub, 128))
                if not first:
                    count = count + t[0, part] * fade
            h[1, part] = peak * scale if last else peak
            t[1, part] = count
        if last:
            top = jnp.transpose(h[1])[0:1]
            count = jnp.sum(jnp.transpose(t[1]), axis=0, keepdims=True)
            if stat is None:
                sent[i, m, rows:] = stats_block(top, count)
            else:
                line = lax.broadcasted_iota(jnp.int32, (8, rows), 0)
                stat[i * 2 + m] = jnp.where(line == 0, top, count)
        else:
            high[i, m] = h[1]
            total[i, m] = t[1]

    def mix(i, m, p, f, out):
        o = jnp.dot(p[...], v[...], preferred_element_type=jnp.float32)
        for g in range(0, o.shape[1], 128):
            part = o[:, g : g + 128]
            if not first:
                part = part + acc_in[i + base, m, :, g : g + 128] * f[...]
            out[i, m, :rows, g : g + 128] = part.astype(out.dtype)

    def run(start, stop, out, stat):
        score(start, 0, s_a)

        def body(i, _):
            score(i, 1, s_b)

            @pl.when(i > start)
            def _():
                mix(i - 1, 1, p_b, f_b, out)

            soft(i, 0, s_a, p_a, f_a, h_a, t_a, stat)
            score(jnp.minimum(i + 1, stop - 1), 0, s_a)
            mix(i, 0, p_a, f_a, out)
            soft(i, 1, s_b, p_b, f_b, h_b, t_b, stat)
            return 0

        lax.fori_loop(start, stop, body, 0)
        mix(stop - 1, 1, p_b, f_b, out)

    if last == "sent":
        run(0, pieces, sent, None)
    elif last == "kept":
        run(0, pieces, kept, kept_stat)
    else:
        run(0, pieces, acc, None)


def attention(qs, kvs, carry, last, base, scale):
    pieces = 2 * len(qs)
    _, _, rows, half = qs[0].shape
    n_keys = sum(kv.shape[0] for kv in kvs)
    width = kvs[0].shape[1] - 2 * half
    vmem = pl.BlockSpec(memory_space=pltpu.VMEM)
    if last == "sent":
        out_shape = [
            jax.ShapeDtypeStruct((pieces, 2, rows + STAT_ROWS, width), jnp.bfloat16),
        ]
    elif last == "kept":
        out_shape = [
            jax.ShapeDtypeStruct((pieces, 2, rows, width), jnp.float32),
            jax.ShapeDtypeStruct((2 * pieces, 8, rows), jnp.float32),
        ]
    else:
        out_shape = [
            jax.ShapeDtypeStruct((pieces, 2, rows, width), jnp.float32),
            jax.ShapeDtypeStruct((pieces, 2, rows, 128), jnp.float32),
            jax.ShapeDtypeStruct((pieces, 2, rows, 128), jnp.float32),
        ]
    n_in = len(qs) + len(kvs)
    aliases = {n_in + i: i for i in range(3)} if carry and not last else {}
    return pl.pallas_call(
        functools.partial(attention_kernel, len(qs), len(kvs), not carry, last, base, scale),
        out_shape=out_shape,
        in_specs=[vmem] * (n_in + len(carry)),
        out_specs=[vmem] * len(out_shape),
        scratch_shapes=[pltpu.VMEM((pieces, 2, rows, half), jnp.bfloat16)]
        + [pltpu.VMEM((n_keys, half), jnp.bfloat16)] * 2
        + [pltpu.VMEM((n_keys, width), jnp.bfloat16)]
        + [pltpu.VMEM((rows, n_keys), jnp.float32)] * 2
        + [pltpu.VMEM((rows, n_keys), jnp.bfloat16)] * 2
        + [pltpu.VMEM((rows, 128), jnp.float32)] * 2
        + [pltpu.VMEM((2, rows, 128), jnp.float32)] * 4,
        input_output_aliases=aliases,
        compiler_params=pltpu.CompilerParams(vmem_limit_bytes=32 * 1024 * 1024),
        cost_estimate=pl.CostEstimate(
            flops=4 * pieces * rows * n_keys * (half + width),
            bytes_accessed=n_keys * (2 * half + width) * 2,
            transcendentals=2 * pieces * rows * n_keys,
        ),
        name="attention",
    )(*qs, *kvs, *carry)


def factors(high_a, total_a, high_b, total_b):
    high = jnp.maximum(high_a, high_b)
    fade_a, fade_b = jnp.exp(high_a - high), jnp.exp(high_b - high)
    return fade_a, fade_b, high, total_a * fade_a + total_b * fade_b


def scaled_sum(a, factor_a, b, factor_b):
    rows = a.shape[0]
    fa = jnp.transpose(jnp.broadcast_to(factor_a, (128, rows)))
    fb = jnp.transpose(jnp.broadcast_to(factor_b, (128, rows)))
    parts = []
    for g in range(0, a.shape[1], 128):
        part = slice(g, g + 128)
        parts.append(a[:, part] * fa + b[:, part].astype(jnp.float32) * fb)
    return parts


def core_merge_kernel(kept, kept_stat, came, own, own_stat, across):
    rows = own.shape[1]
    line = lax.broadcasted_iota(jnp.int32, (8, rows), 0)
    for i, out in enumerate((own, across)):
        for m in range(2):
            at = 2 * i + m
            stats = stats_rows(came[i, m, rows:])
            fa, fb, high, total = factors(kept_stat[at, 0:1], kept_stat[at, 1:2], *stats)
            parts = scaled_sum(kept[i, m], fa, came[i, m, :rows], fb)
            for g, part in enumerate(parts):
                out[m, :rows, g * 128 : (g + 1) * 128] = part.astype(out.dtype)
            if i == 0:
                own_stat[m] = jnp.where(line == 0, high, total)
            else:
                across[m, rows:] = stats_block(high, total)


def core_merged(kept, kept_stat, came):
    _, _, rows, width = kept.shape
    vmem = pl.BlockSpec(memory_space=pltpu.VMEM)
    return pl.pallas_call(
        core_merge_kernel,
        out_shape=[
            jax.ShapeDtypeStruct((2, rows, width), jnp.float32),
            jax.ShapeDtypeStruct((2, 8, rows), jnp.float32),
            jax.ShapeDtypeStruct((2, rows + STAT_ROWS, width), jnp.bfloat16),
        ],
        in_specs=[vmem] * 3,
        out_specs=[vmem] * 3,
        compiler_params=pltpu.CompilerParams(vmem_limit_bytes=8 * 1024 * 1024),
        name="core_merge",
    )(kept, kept_stat, came)


def project_kernel(own, own_stat, came, diff_scale, gain, w_out, shares, head_out):
    rows, heads = shares.shape[0], diff_scale.shape[0]
    width = own.shape[2]
    maps = []
    for m in range(2):
        each = own.shape[1]
        stats = stats_rows(came[m, each:])
        fa, fb, _, total = factors(own_stat[m, 0:1], own_stat[m, 1:2], *stats)
        maps.append(scaled_sum(own[m], fa / total, came[m, :each], fb / total))
    for h in range(heads):
        part = slice(h * rows, (h + 1) * rows)
        mixed = [a[part] - diff_scale[h] * b[part] for a, b in zip(*maps)]
        mean = sum(jnp.sum(x * x, axis=1, keepdims=True) for x in mixed) / width
        norm = lax.rsqrt(mean + EPS)
        for g, x in enumerate(mixed):
            at = slice(h * width + g * 128, h * width + (g + 1) * 128)
            x = x * norm * gain[:, g * 128 : (g + 1) * 128]
            head_out[:, at] = x.astype(jnp.bfloat16)
    out = jnp.dot(head_out[...], w_out[...], preferred_element_type=jnp.float32)
    shares[...] = out.astype(jnp.bfloat16)


def projected(own, own_stat, came, diff_scale, gain, w_out, rows):
    vmem = pl.BlockSpec(memory_space=pltpu.VMEM)
    smem = pl.BlockSpec(memory_space=pltpu.SMEM)
    return pl.pallas_call(
        project_kernel,
        out_shape=jax.ShapeDtypeStruct((rows, w_out.shape[1]), jnp.bfloat16),
        in_specs=[vmem] * 3 + [smem, vmem, vmem],
        out_specs=vmem,
        scratch_shapes=[pltpu.VMEM((rows, w_out.shape[0]), jnp.bfloat16)],
        compiler_params=pltpu.CompilerParams(vmem_limit_bytes=12 * 1024 * 1024),
        name="project",
    )(own, own_stat, came, diff_scale, gain, w_out)


LANES = 128


def settle_kernel(parts, residual, gain, token, state, *refs):
    out, normed, tiles = refs
    rows, width = residual.shape
    high = width // LANES
    step = 16
    for r in range(0, rows, step):
        x = residual[r : r + step].astype(jnp.float32)
        share = parts[0, r : r + step].astype(jnp.float32)
        for p in range(1, parts.shape[0]):
            share = share + parts[p, r : r + step].astype(jnp.float32)
        x = x + share
        n = x * lax.rsqrt(jnp.mean(x * x, axis=1, keepdims=True) + EPS) * gain[...]
        for j in range(high):
            at = pl.ds(r * high + j, step, stride=high)
            state[at] = x[:, j * LANES : (j + 1) * LANES]
            normed[at] = n[:, j * LANES : (j + 1) * LANES]
    tiles[...] = normed[...].astype(jnp.bfloat16)
    places, slots = out.shape[0], out.shape[1] // high

    def lay(e, _):
        for s in range(slots):
            t = pl.multiple_of(token[e * slots + s] * high, high)
            out[e, s * high : (s + 1) * high] = tiles[pl.ds(t, high)]
        return 0

    lax.fori_loop(0, places, lay, 0, unroll=8)


def settled(parts, residual, gain, token, places, slots):
    rows, width = residual.shape
    high = width // LANES
    vmem = pl.BlockSpec(memory_space=pltpu.VMEM)
    smem = pl.BlockSpec(memory_space=pltpu.SMEM)
    return pl.pallas_call(
        settle_kernel,
        out_shape=[jax.ShapeDtypeStruct((rows * high, LANES), jnp.float32)]
        + [jax.ShapeDtypeStruct((places, slots * high, LANES), jnp.bfloat16)],
        in_specs=[vmem, vmem, vmem, smem],
        out_specs=[vmem] * 2,
        scratch_shapes=[
            pltpu.VMEM((rows * high, LANES), jnp.float32),
            pltpu.VMEM((rows * high, LANES), jnp.bfloat16),
        ],
        compiler_params=pltpu.CompilerParams(vmem_limit_bytes=6 * 1024 * 1024),
        name="settle",
    )(parts, residual, gain, token)


def tiled_kernel(parts, residual, state):
    rows, width = residual.shape
    high = width // LANES
    x = residual[...].astype(jnp.float32)
    share = parts[0].astype(jnp.float32)
    for p in range(1, parts.shape[0]):
        share = share + parts[p].astype(jnp.float32)
    x = x + share
    for j in range(high):
        state[pl.ds(j, rows, stride=high)] = x[:, j * LANES : (j + 1) * LANES]


def tiled(parts, residual):
    rows, width = residual.shape
    vmem = pl.BlockSpec(memory_space=pltpu.VMEM)
    return pl.pallas_call(
        tiled_kernel,
        out_shape=jax.ShapeDtypeStruct((rows * width // LANES, LANES), jnp.float32),
        in_specs=[vmem] * 2,
        out_specs=vmem,
        compiler_params=pltpu.CompilerParams(vmem_limit_bytes=6 * 1024 * 1024),
        name="tiled",
    )(parts, residual)


def expert_kernel(count, *refs):
    blocks, (w_gate, w_up, w_down) = refs[:count], refs[count : count + 3]
    outs, (x, wide) = refs[count + 3 : 2 * count + 3], refs[2 * count + 3 :]
    high = blocks[0].shape[1]
    at = 0
    for block in blocks:
        n = block.shape[0]
        wide[: n * high] = block[...].reshape(n * high, LANES).astype(jnp.float32)
        for j in range(high):
            column = wide[pl.ds(j, n, stride=high)]
            x[at : at + n, j * LANES : (j + 1) * LANES] = column.astype(jnp.bfloat16)
        at += n
    gate = jnp.dot(x[...], w_gate[...], preferred_element_type=jnp.float32)
    up = jnp.dot(x[...], w_up[...], preferred_element_type=jnp.float32)
    hidden = (gate / (1.0 + jnp.exp(-gate)) * up).astype(jnp.bfloat16)
    result = jnp.dot(hidden, w_down[...], preferred_element_type=jnp.float32)
    at = 0
    for out in outs:
        n = out.shape[0]
        for j in range(high):
            wide[pl.ds(j, n, stride=high)] = result[at : at + n, j * LANES : (j + 1) * LANES]
        out[...] = wide[: n * high].astype(jnp.bfloat16).reshape(n, high, LANES)
        at += n


def expert(blocks, w_gate, w_up, w_down):
    total = sum(b.shape[0] for b in blocks)
    most = max(b.shape[0] for b in blocks)
    high = blocks[0].shape[1]
    vmem = pl.BlockSpec(memory_space=pltpu.VMEM)
    return pl.pallas_call(
        functools.partial(expert_kernel, len(blocks)),
        out_shape=[jax.ShapeDtypeStruct(b.shape, jnp.bfloat16) for b in blocks],
        in_specs=[vmem] * (len(blocks) + 3),
        out_specs=[vmem] * len(blocks),
        scratch_shapes=[
            pltpu.VMEM((total, high * LANES), jnp.bfloat16),
            pltpu.VMEM((most * high, LANES), jnp.float32),
        ],
        compiler_params=pltpu.CompilerParams(vmem_limit_bytes=24 * 1024 * 1024),
        cost_estimate=pl.CostEstimate(
            flops=6 * total * high * LANES * w_up.shape[1],
            bytes_accessed=2 * total * high * LANES * 2,
            transcendentals=total * w_up.shape[1],
        ),
        name="expert",
    )(*blocks, w_gate, w_up, w_down)


def finish_kernel(slots, top, state, place, weight, *refs):
    returned, out, wide = refs
    rows, width = out.shape
    high = width // LANES

    def add(t, _):
        at = pl.ds(pl.multiple_of(t * high, high), high)
        y = state[at]
        for r in range(top):
            k = t * top + r
            y = y + weight[k] * returned[place[k]].astype(jnp.float32)
        wide[at] = y
        return 0

    lax.fori_loop(0, rows, add, 0, unroll=4)
    step = 16
    for r in range(0, rows, step):
        for j in range(high):
            column = wide[pl.ds(r * high + j, step, stride=high)]
            out[r : r + step, j * LANES : (j + 1) * LANES] = column.astype(jnp.bfloat16)


def finished(state, returned, place, weight, rows, top):
    high = returned.shape[1]
    vmem = pl.BlockSpec(memory_space=pltpu.VMEM)
    smem = pl.BlockSpec(memory_space=pltpu.SMEM)
    return pl.pallas_call(
        functools.partial(finish_kernel, 1, top),
        out_shape=jax.ShapeDtypeStruct((rows, high * LANES), jnp.bfloat16),
        in_specs=[vmem, smem, smem, vmem],
        out_specs=vmem,
        scratch_shapes=[pltpu.VMEM((rows * high, LANES), jnp.float32)],
        compiler_params=pltpu.CompilerParams(vmem_limit_bytes=6 * 1024 * 1024),
        name="finish",
    )(state, place, weight, returned)


def served(block, weights):
    half = block.shape[0] // 2
    behind, ahead = shifted(block, TP, 1), shifted(block, TP, -1)
    near = expert([block], *weights)
    behind, ahead, *near = lax.optimization_barrier((behind, ahead, *near))
    far = [shifted(behind[:half], TP, 1), shifted(ahead[half:], TP, -1)]
    return [*near, *expert([behind, ahead], *weights), *expert(far, *weights)]


def summed_around(parts):
    own, behind, ahead, first, second = (p.astype(jnp.float32) for p in parts)
    half = parts[3].shape[0]
    first, second = shifted(parts[3], TP, 1), shifted(parts[4], TP, -1)
    zero = jnp.zeros(first.shape, jnp.float32)
    ahead = ahead + jnp.concatenate([first.astype(jnp.float32), zero])
    behind = behind + jnp.concatenate([zero, second.astype(jnp.float32)])
    from_behind = shifted(ahead.astype(jnp.bfloat16), TP, 1)
    from_ahead = shifted(behind.astype(jnp.bfloat16), TP, -1)
    total = own + from_behind.astype(jnp.float32) + from_ahead.astype(jnp.float32)
    return total.astype(jnp.bfloat16)


def exchanged(x):
    return lax.all_to_all(x, SP, split_axis=0, concat_axis=0, tiled=True)


def local(
    queries,
    keys,
    values,
    diff_scale,
    head_gain,
    w_out,
    residual,
    norm_gain,
    route_ids,
    route_weights,
    w_gate,
    w_up,
    w_down,
):
    q_rows = queries.shape[0]
    heads_dev = diff_scale.shape[0]
    half_dim = queries.shape[1] // (2 * heads_dev)
    group_cols = keys.shape[1] // KV_HEADS
    value_cols = values.shape[1] // KV_HEADS
    swap = [(0, 1), (1, 0)]

    group, quarter = lax.axis_index("xh"), lax.axis_index("xl")
    part_rows = q_rows // 2

    def own_part(x, cols):
        x = jnp.where(group == 0, x[:, :cols], x[:, cols:])
        return jnp.where(quarter == 0, x[:part_rows], x[part_rows:])

    k_part, v_part = own_part(keys, group_cols), own_part(values, value_cols)
    joined = jnp.concatenate([k_part, v_part], axis=1)
    q_own = jnp.stack(
        [
            jnp.concatenate(
                [
                    queries[:, (2 * h + m) * half_dim : (2 * h + m + 1) * half_dim]
                    for h in range(heads_dev)
                ]
            )
            for m in range(2)
        ]
    )

    joined, q_own = lax.optimization_barrier((joined, q_own))
    copies = jnp.broadcast_to(joined, (lax.axis_size("y"), *joined.shape))
    block = lax.all_to_all(copies, "y", split_axis=0, concat_axis=0, tiled=True)
    block = block.reshape(-1, joined.shape[1])
    q_x = lax.ppermute(q_own, "xl", swap)
    block, q_x = lax.optimization_barrier((block, q_x))
    q_pair = jnp.stack([q_own, q_x])
    q_other = lax.ppermute(q_pair, "core", swap)
    qs = [q_pair, q_other]
    scale = 1.0 / math.sqrt(half_dim)
    n = lax.axis_size("z")
    right, left = shifted(block, "z", 1), shifted(block, "z", -1)
    kvs, carry = [block, right, left], []
    for step in range(2, n // 2 + 1):
        if step == n // 2:
            right, left = shifted(right, "z", 1), None
        else:
            right, left = shifted(right, "z", 1), shifted(left, "z", -1)
        carry = attention(qs, kvs, carry, "", 0, scale)
        kvs = [kv for kv in (right, left) if kv is not None]
        kvs, carry = lax.optimization_barrier((kvs, carry))
        right, left = kvs[0], kvs[-1]
    (sent,) = attention(qs[1:], kvs, carry, "sent", 2, scale)
    sent, *carry = lax.optimization_barrier((sent, *carry))
    sent = lax.ppermute(sent, "core", swap)
    kept, kept_stat = attention(qs[:1], kvs, carry, "kept", 0, scale)
    own, own_stat, across = core_merged(kept, kept_stat, sent)
    came = lax.ppermute(across, "xl", swap)
    shares = projected(own, own_stat, came, diff_scale, head_gain[None, :], w_out, q_rows)
    rows_out = residual.shape[0]
    arrived = lax.all_to_all(
        cut_along(shares, 0, lax.axis_size(TP)), TP, split_axis=0, concat_axis=0, tiled=True
    )
    places = lax.axis_size(SP)
    top = route_ids.shape[1]
    slots = 2
    flat_ids = route_ids.reshape(-1)
    onehot = (flat_ids[:, None] == jnp.arange(places, dtype=jnp.int32)[None, :]).astype(jnp.int32)
    slot = jnp.sum((jnp.cumsum(onehot, axis=0) - onehot) * onehot, axis=1)
    dest = flat_ids * slots + slot
    taken = dest[:, None] == jnp.arange(places * slots, dtype=jnp.int32)[None, :]
    source = jnp.arange(flat_ids.shape[0], dtype=jnp.int32)[:, None] // top
    token = jnp.sum(jnp.where(taken, source, 0), axis=0)

    _, outgoing = settled(arrived, residual, norm_gain[None, :], token, places, slots)
    high = outgoing.shape[1] // slots
    received, state = lax.optimization_barrier((exchanged(outgoing), tiled(arrived, residual)))
    received = received.reshape(places * slots, high, LANES)
    parts = served(received, (w_gate[0], w_up[0], w_down[0]))
    back = summed_around(parts).reshape(places, slots * high, LANES)
    returned = exchanged(back).reshape(places * slots, high, LANES)
    place = dest
    return finished(state, returned, place, route_weights.reshape(-1), rows_out, top)


def solution(mesh):
    cells = mesh.devices.reshape(8, 4, 2, 2, 2)
    mesh = Mesh(cells, ("z", "y", "core", "xh", "xl"))
    in_specs = (
        P(SP, TP),
        P(SP, None),
        P(SP, None),
        P(TP),
        P(),
        P(TP, None),
        P(SP + TP, None),
        P(),
        P(SP + TP, None),
        P(SP + TP, None),
        P(SP, None, TP),
        P(SP, None, TP),
        P(SP, TP, None),
    )
    out_specs = P(SP + TP, None)
    return jax.shard_map(local, mesh=mesh, in_specs=in_specs, out_specs=out_specs, check_vma=False)
```
